512 devices in a mesh: grp: 2 (over y), sp: 64 (over z, core), tp: 4 (over x).
Axes of the slice: x: 4, y: 2, z: 32, core: 2. Of those that a mesh axis runs over, the one named last changes fastest.
The devices are a block of a 4x8x32 slice.
Arguments:
- recurrent_query: bfloat16 [32768, 1024], P(('grp', 'sp'), 'tp'), parts along dimension 0, may hold values from -6 to 6
- recurrent_forget_gate: bfloat16 [32768, 1024], P(('grp', 'sp'), 'tp'), parts along dimension 0, may hold values from -4.5 to 4.5
- recurrent_value: bfloat16 [32768, 1024], P(('grp', 'sp'), 'tp'), parts along dimension 0, may hold values from -6 to 6
- recurrent_gate_lower_bound: float32 [1024], P('tp'), may hold values from 1.5 to 14
- recurrent_added_decay: float32 [32768, 8], P(('grp', 'sp'), 'tp'), parts along dimension 0, may hold values from -0.51 to 0
- recurrent_norm_gain: float32 [128], replicated, may hold values from 0.1 to 1.9
- attention_query_first: bfloat16 [32768, 512], P(('grp', 'sp'), 'tp'), parts along dimension 0, may hold values from -20 to 20
- attention_key_first: bfloat16 [32768, 256], P(('grp', 'sp'), 'tp'), parts along dimension 0, may hold values from -20 to 20
- attention_query_second: bfloat16 [32768, 512], P(('grp', 'sp'), 'tp'), parts along dimension 0, may hold values from -20 to 20
- attention_key_second: bfloat16 [32768, 256], P(('grp', 'sp'), 'tp'), parts along dimension 0, may hold values from -20 to 20
- attention_value: bfloat16 [32768, 512], P(('grp', 'sp'), 'tp'), parts along dimension 0, may hold values from -6 to 6
- second_map_weight: float32 [8], P('tp'), may hold values from 0.3 to 0.8
- attention_norm_gain: float32 [128], replicated, may hold values from 0.1 to 1.9
- output_weight: bfloat16 [2, 1024, 2048], P(None, 'tp', 'sp'), may hold values from -0.125 to 0.125
Outputs:
- mixed: bfloat16 [32768, 2048], P(('grp', 'sp', 'tp')), parts along dimension 0
The draws below stay inside these ranges and needn't reach their ends.
There are 2 independent parts, one for each index of `grp`. The reference program is written for one: setup_inputs(seed, part) draws one part's arguments, and reference() takes and returns one part's arrays. A program takes and returns all parts, laid end to end along the dimension named above; an argument that names none is the same for every part. Nothing has to cross between parts.
All inputs are finite; a program needn't handle non-finite values.
Results may differ from the reference program's by a relative error of at most 0.02.
Values may be sent and summed in bfloat16 or wider, within the bound.
A program may use at most 64 MiB of HBM per device.

```python
import jax
import jax.numpy as jnp
from jax import lax

D = 2048
RECURRENT_HEADS = 8
HG_DK = 128
HG_DV = 128
DA_HEADS = 8
KV_HEADS = 4
DA_HD = 64
BLK = 32
TOK_DEV = 256
TOKENS = 16384
MIX_WIDTH = 1024
N_TP = 4


def loguniform_draw(key, shape, low, high):
    return jnp.exp(jax.random.uniform(key, shape, jnp.float32, jnp.log(low), jnp.log(high)))


def draw_recurrent_gate_lower_bound(key, part):
    split_keys = jax.random.split(key, 4)
    order = jax.random.permutation(split_keys[0], RECURRENT_HEADS)
    fast = order < RECURRENT_HEADS // 2
    fast_rate = loguniform_draw(split_keys[1], (RECURRENT_HEADS,), 0.04, 0.12)
    slow_rate = loguniform_draw(split_keys[2], (RECURRENT_HEADS,), 0.3, 1.2) / TOKENS
    jitter = loguniform_draw(split_keys[3], (RECURRENT_HEADS, HG_DK), 0.7, 1.4)
    floor_rate = jnp.where(fast, fast_rate, slow_rate)[:, None] * jitter
    return jnp.log(1.0 / floor_rate - 1.0).reshape(-1).astype(jnp.float32)


def draw_recurrent_forget_gate(key, part):
    split_keys = jax.random.split(key, 2)
    block_count = TOKENS // TOK_DEV
    shift = jax.random.uniform(split_keys[0], (block_count, 1, RECURRENT_HEADS, 1), jnp.float32, -1.5, 1.5)
    rough = jax.random.truncated_normal(split_keys[1], -3.0, 3.0, (block_count, TOK_DEV, RECURRENT_HEADS, HG_DK), jnp.float32)
    return (rough + shift).reshape(TOKENS, RECURRENT_HEADS * HG_DK).astype(jnp.bfloat16)


def draw_recurrent_added_decay(key, part):
    split_keys = jax.random.split(key, 2)
    spots = jax.random.randint(split_keys[0], (3, RECURRENT_HEADS), 0, TOKENS)
    depth = jax.random.uniform(split_keys[1], (3, RECURRENT_HEADS), jnp.float32, -0.51, -0.22)
    matches = jnp.arange(TOKENS)[:, None, None] == spots[None]
    return jnp.min(jnp.where(matches, depth[None], 0.0), axis=1).astype(jnp.float32)


def draw_pair(key, marker):
    base = jax.random.fold_in(key, marker)
    split_keys = jax.random.split(base, 2)
    queries = 1.3 * jax.random.truncated_normal(split_keys[0], -6.0, 6.0, (TOKENS, DA_HEADS * DA_HD), jnp.float32)
    key_rows = 1.3 * jax.random.truncated_normal(split_keys[1], -6.0, 6.0, (TOKENS, KV_HEADS * DA_HD), jnp.float32)
    return (queries.astype(jnp.bfloat16), key_rows.astype(jnp.bfloat16))


def draw_attention_query_first(key, part):
    return draw_pair(key, 11)[0]


def draw_attention_key_first(key, part):
    return draw_pair(key, 11)[1]


def draw_attention_query_second(key, part):
    return draw_pair(key, 12)[0]


def draw_attention_key_second(key, part):
    return draw_pair(key, 12)[1]


def shard_levels(stream_key, shape, pieces, smallest, high):
    def one(axis_at, shards_of):
        draws = jax.random.uniform(jax.random.fold_in(jax.random.fold_in(stream_key, 6), axis_at), (shards_of,), jnp.float32, smallest / len(pieces), high / len(pieces))
        return jnp.repeat(jnp.exp(draws), shape[axis_at] // shards_of).reshape((-1,) + (1,) * (len(shape) - axis_at - 1))

    loudness = one(*pieces[0])
    for cut in pieces[1:]:
        loudness = loudness * one(*cut)
    return loudness


def scatter_about(rng, extent, width, most, cuts=(), held_as=jnp.bfloat16):
    loudness = shard_levels(rng, extent, cuts, -0.22, 0.18) if cuts else 1.0
    array = jax.random.normal(rng, extent, jnp.float32) * width * loudness
    return jnp.minimum(jnp.maximum(array, -most), most).astype(held_as)


def setup_inputs(seed: int = 0, part: int = 0) -> dict:
    keys = jax.random.split(jax.random.key(seed), 15)
    own_keys = jax.random.split(jax.random.fold_in(keys[14], part), 15)
    recurrent_query = scatter_about(own_keys[0], (TOKENS, RECURRENT_HEADS * HG_DK), 1.0, 6.0, ((0, 64), (1, 4)))
    recurrent_forget_gate = draw_recurrent_forget_gate(jax.random.fold_in(jax.random.fold_in(keys[14], part), 71), part)
    recurrent_value = scatter_about(own_keys[2], (TOKENS, MIX_WIDTH), 1.0, 6.0, ((0, 64), (1, 4)))
    recurrent_gate_lower_bound = draw_recurrent_gate_lower_bound(jax.random.fold_in(keys[14], 71), part)
    recurrent_added_decay = draw_recurrent_added_decay(jax.random.fold_in(jax.random.fold_in(keys[14], part), 71), part)
    recurrent_norm_gain = jnp.clip(1.0 + 0.18 * jax.random.normal(keys[5], (HG_DV,), jnp.float32), 0.1, 1.9)
    attention_query_first = draw_attention_query_first(jax.random.fold_in(jax.random.fold_in(keys[14], part), 71), part)
    attention_key_first = draw_attention_key_first(jax.random.fold_in(jax.random.fold_in(keys[14], part), 71), part)
    attention_query_second = draw_attention_query_second(jax.random.fold_in(jax.random.fold_in(keys[14], part), 71), part)
    attention_key_second = draw_attention_key_second(jax.random.fold_in(jax.random.fold_in(keys[14], part), 71), part)
    attention_value = scatter_about(own_keys[10], (TOKENS, KV_HEADS * 2 * DA_HD), 1.0, 6.0, ((0, 64), (1, 4)))
    second_map_weight = jnp.clip(0.3 + 0.5 * jax.random.uniform(keys[11], (DA_HEADS,), jnp.float32) ** shard_levels(keys[11], (DA_HEADS,), ((0, 4),), -0.2, 0.2), 0.3, 0.8)
    attention_norm_gain = jnp.clip(1.0 + 0.18 * jax.random.normal(keys[12], (2 * DA_HD,), jnp.float32), 0.1, 1.9)
    output_weight = scatter_about(keys[13], (2, MIX_WIDTH, D), (2 * MIX_WIDTH) ** -0.5, 0.125, ((1, 4), (2, 64)))
    return dict(recurrent_query=recurrent_query, recurrent_forget_gate=recurrent_forget_gate, recurrent_value=recurrent_value, recurrent_gate_lower_bound=recurrent_gate_lower_bound, recurrent_added_decay=recurrent_added_decay, recurrent_norm_gain=recurrent_norm_gain, attention_query_first=attention_query_first, attention_key_first=attention_key_first, attention_query_second=attention_query_second, attention_key_second=attention_key_second, attention_value=attention_value, second_map_weight=second_map_weight, attention_norm_gain=attention_norm_gain, output_weight=output_weight)


epsilon = 1e-06
highest = lax.Precision.HIGHEST

def head_norm(head_values, gain_vec):
    mean_square = lax.optimization_barrier(jnp.mean(head_values * head_values, axis=-1, keepdims=True))
    return head_values * lax.rsqrt(mean_square + epsilon) * gain_vec

def decay_factors(gate_preactivation, lower_bound_logit, added_log_decay, number_of_heads):
    token_count = gate_preactivation.shape[0]
    floor_rate = jax.nn.sigmoid(-lower_bound_logit).reshape(number_of_heads, -1)
    state_inflow = floor_rate[None] * jax.nn.sigmoid(-gate_preactivation.astype(jnp.float32)).reshape(token_count, number_of_heads, -1)
    decay_logarithm = jnp.log1p(-state_inflow) + added_log_decay[:, :, None]
    return (state_inflow, decay_logarithm)

def recurrence_blocks(queries, decay_logarithm, state_inflow, value_rows, block_len):
    token_count, number_of_heads, key_width = queries.shape
    block_count = token_count // block_len

    def to_blocks(source):
        return source.reshape(block_count, block_len, number_of_heads, source.shape[-1])
    causal = jnp.tril(jnp.ones((block_len, block_len), jnp.float32))[:, :, None, None]

    def block_step(carry_state, inputs):
        query_blk, decay_blk, inflow_blk, value_blk = inputs
        cumulative = jnp.cumsum(decay_blk, axis=0)
        relative = cumulative[:, None] - cumulative[None, :]
        decay_table = jnp.exp(jnp.minimum(relative, 0.0)) * causal
        scores = jnp.einsum('thd,shd,tshd->hts', query_blk, inflow_blk, decay_table, precision=highest)
        block_out = jnp.einsum('hts,shv->thv', scores, value_blk, precision=highest)
        block_out = block_out + jnp.einsum('thd,hdv->thv', query_blk * jnp.exp(cumulative), carry_state, precision=highest)
        last_log = cumulative[-1]
        new_state = jnp.exp(last_log)[:, :, None] * carry_state + jnp.einsum('shd,shv->hdv', inflow_blk * jnp.exp(last_log[None] - cumulative), value_blk, precision=highest)
        return (new_state, block_out)
    zero_state = jnp.zeros((number_of_heads, key_width, value_rows.shape[-1]), jnp.float32)
    final_state, outputs = lax.scan(block_step, zero_state, (to_blocks(queries), to_blocks(decay_logarithm), to_blocks(state_inflow), to_blocks(value_rows)))
    return (final_state, outputs.reshape(token_count, number_of_heads, -1))

def recurrent_token_mixer(recurrent_query, recurrent_forget_gate, recurrent_value, recurrent_gate_lower_bound, recurrent_added_decay, recurrent_norm_gain):
    token_count = recurrent_query.shape[0]
    state_inflow, decay_logarithm = decay_factors(recurrent_forget_gate, recurrent_gate_lower_bound, recurrent_added_decay, RECURRENT_HEADS)
    queries = recurrent_query.astype(jnp.float32).reshape(token_count, RECURRENT_HEADS, HG_DK)
    value_rows = recurrent_value.astype(jnp.float32).reshape(token_count, RECURRENT_HEADS, HG_DV)
    unused, mixed_rows = recurrence_blocks(queries, decay_logarithm, state_inflow, value_rows, BLK)
    return head_norm(mixed_rows, recurrent_norm_gain).astype(jnp.bfloat16)

def difference_mixer(attention_query_first, attention_key_first, attention_query_second, attention_key_second, attention_value, second_map_weight, attention_norm_gain):
    token_count = attention_query_first.shape[0]
    group_size = DA_HEADS // KV_HEADS
    score_scale = DA_HD ** (-0.5)
    keys_one = attention_key_first.astype(jnp.float32).reshape(token_count, KV_HEADS, DA_HD)
    keys_two = attention_key_second.astype(jnp.float32).reshape(token_count, KV_HEADS, DA_HD)
    value_rows = attention_value.astype(jnp.float32).reshape(token_count, KV_HEADS, 2 * DA_HD)
    lambda_table = second_map_weight.reshape(KV_HEADS, group_size)
    key_pos = jnp.arange(token_count).astype(jnp.int32)

    def per_block(block_index):
        first_row = (block_index * TOK_DEV).astype(jnp.int32)
        query_pos = first_row + jnp.arange(TOK_DEV).astype(jnp.int32)
        allowed = key_pos[None, :] <= query_pos[:, None]

        def slice_queries(source):
            picked = lax.dynamic_slice_in_dim(source, first_row, TOK_DEV, 0)
            return picked.astype(jnp.float32).reshape(TOK_DEV, KV_HEADS, group_size, DA_HD)
        queries_one = slice_queries(attention_query_first)
        queries_two = slice_queries(attention_query_second)

        def per_head(head_index):
            results = []
            for queries, key_rows in ((queries_one, keys_one), (queries_two, keys_two)):
                scores = jnp.einsum('qgd,sd->gqs', queries[:, head_index], key_rows[:, head_index], precision=highest) * score_scale
                scores = jnp.where(allowed[None], scores, -1e+30)
                row_max = lax.optimization_barrier(jnp.max(scores, axis=-1, keepdims=True))
                weights = jnp.where(allowed[None], jnp.exp(scores - row_max), 0.0)
                weight_mass = lax.optimization_barrier(jnp.sum(weights, axis=-1))
                rounded = lax.optimization_barrier(weights.astype(jnp.bfloat16)).astype(jnp.float32)
                product = jnp.einsum('gqs,sv->gqv', rounded, value_rows[:, head_index], precision=highest)
                results.append(product / weight_mass[..., None])
            return results[0] - lambda_table[head_index][:, None, None] * results[1]
        heads_out = lax.map(per_head, jnp.arange(KV_HEADS).astype(jnp.int32))
        return jnp.transpose(heads_out, (2, 0, 1, 3)).reshape(TOK_DEV, DA_HEADS, 2 * DA_HD)
    blocks = lax.map(per_block, jnp.arange(token_count // TOK_DEV).astype(jnp.int32))
    mixed_rows = blocks.reshape(token_count, DA_HEADS, 2 * DA_HD)
    return head_norm(mixed_rows, attention_norm_gain).astype(jnp.bfloat16)

def reference(recurrent_query, recurrent_forget_gate, recurrent_value, recurrent_gate_lower_bound, recurrent_added_decay, recurrent_norm_gain, attention_query_first, attention_key_first, attention_query_second, attention_key_second, attention_value, second_map_weight, attention_norm_gain, output_weight):
    recurrent_output = recurrent_token_mixer(recurrent_query, recurrent_forget_gate, recurrent_value, recurrent_gate_lower_bound, recurrent_added_decay, recurrent_norm_gain)
    attended = difference_mixer(attention_query_first, attention_key_first, attention_query_second, attention_key_second, attention_value, second_map_weight, attention_norm_gain)
    token_count = recurrent_query.shape[0]
    rec_share = RECURRENT_HEADS // N_TP
    att_share = DA_HEADS // N_TP
    row_share = MIX_WIDTH // N_TP
    summed = jnp.zeros((token_count, D), jnp.float32)
    for member in range(N_TP):
        rec_part = recurrent_output[:, member * rec_share:(member + 1) * rec_share].reshape(token_count, -1)
        att_part = attended[:, member * att_share:(member + 1) * att_share].reshape(token_count, -1)
        rows_rec = output_weight[0, member * row_share:(member + 1) * row_share]
        rows_att = output_weight[1, member * row_share:(member + 1) * row_share]
        partial_term = jnp.dot(rec_part, rows_rec, preferred_element_type=jnp.float32) + jnp.dot(att_part, rows_att, preferred_element_type=jnp.float32)
        summed = summed + lax.optimization_barrier(partial_term.astype(jnp.bfloat16)).astype(jnp.float32)
    return summed.astype(jnp.bfloat16)
```

```python
import functools

import jax
import jax.numpy as jnp
from jax import lax
from jax.experimental import pallas as pl
from jax.experimental.pallas import tpu as pltpu
from jax.sharding import PartitionSpec as P

HEAD = 128
DA_HD = 64
BLK = 64
HOPS = 4
EPS = 1e-06
f32, bf16 = jnp.float32, jnp.bfloat16
NT = (((1,), (1,)), ((), ()))
TN = (((0,), (0,)), ((), ()))


def dot(a, b, dims=(((1,), (0,)), ((), ())), precision=None):
    return lax.dot_general(a, b, dims, precision=precision, preferred_element_type=f32)


def kernel(
    nz, kvl, wl, qp, rq, fg, rv, lb, added, lam, rgain, again, out,
    kv, wbuf, acc, mrow, sown, spart, tm, ch, pe, loc, qe, dev_state, dev_decay,
    arec, aatt, ract, part,
    copy_sem, send_sem, kvz_sem, kvp_sem, wz_sem, wx_sem, wr_sem, wp_sem, st_sem, act_sem,
):
    g, sp, x = lax.axis_index("grp"), lax.axis_index("sp"), lax.axis_index("tp")
    ntp = lax.axis_size("tp")
    z, c = sp // 2, sp % 2
    half = nz // 2
    kv_reach = (half - 1, half)
    w_reach = (half, half - 1)
    tok = rq.shape[0]
    rows_out = tok // ntp

    def zdev(dz):
        return (g, ((z + dz + nz) % nz) * 2 + c, x)

    def xdev(dx):
        return (g, sp, (x + dx + ntp) % ntp)

    partner = (g, z * 2 + 1 - c, x)
    ring = (zdev(1), zdev(-1))

    def send(src, dst, s_sem, r_sem, to):
        pltpu.make_async_remote_copy(
            src_ref=src, dst_ref=dst, send_sem=s_sem, recv_sem=r_sem,
            device_id=to, device_id_type=pl.DeviceIdType.MESH,
        ).start()

    def got(ref, sem):
        pltpu.make_async_copy(ref, ref, sem).wait()

    def chip_at(d, i):
        return (z - i + nz) % nz if d == 0 else (z + i) % nz

    cp_kv = pltpu.make_async_copy(kvl, kv.at[sp], copy_sem.at[0])
    cp_w = pltpu.make_async_copy(wl, wbuf.at[0, sp], copy_sem.at[1])
    cp_kv.start()
    cp_w.start()
    tm[...] = jnp.zeros_like(tm)
    ch[...] = jnp.zeros_like(ch)

    barrier = pltpu.get_barrier_semaphore()
    near = [zdev(1), zdev(-1), zdev(HOPS), zdev(-HOPS), xdev(1), xdev(2), xdev(3), partner]
    for dev in near:
        pl.semaphore_signal(barrier, inc=1, device_id=dev, device_id_type=pl.DeviceIdType.MESH)
    pl.semaphore_wait(barrier, len(near))

    s_kvz, s_kvp, s_wz, s_wx, s_wr, s_wp, s_act, s_own, s_chain, s_pe = (
        send_sem.at[k] for k in range(10)
    )
    s_tm = [send_sem.at[10 + r] for r in range(HOPS)]

    cp_kv.wait()
    for kind in range(2):
        mine = kv.at[sp, kind]
        send(mine, mine, s_kvz, kvz_sem.at[0, kind], ring[0])
        send(mine, mine, s_kvz, kvz_sem.at[1, kind], ring[1])
    for kind in range(2):
        mine = kv.at[sp, kind]
        send(mine, mine, s_kvp, kvp_sem.at[0, 2 * half + kind], partner)
    cp_w.wait()
    mine = wbuf.at[0, sp]
    send(mine, mine, s_wz, wz_sem.at[0, 1], ring[0])
    send(mine, mine, s_wz, wz_sem.at[1, 1], ring[1])
    send(mine, wbuf.at[3, sp], s_wx, wx_sem.at[1, 0, 0], xdev(1))
    send(mine, wbuf.at[1, sp], s_wx, wx_sem.at[0, 0, 0], xdev(-1))
    send(mine, mine, s_wp, wp_sem.at[0], partner)

    floor_rate = jax.nn.sigmoid(-lb[...])
    inflow = floor_rate * jax.nn.sigmoid(-fg[...].astype(f32))
    one_less = 1.0 - inflow
    add2 = added[...]
    add_wide = jnp.concatenate(
        [jnp.broadcast_to(add2[:, h : h + 1], (tok, HEAD)) for h in range(2)], axis=1
    )
    log_decay = jnp.log(one_less) - ((one_less - 1.0) + inflow) / one_less + add_wide
    row = lax.broadcasted_iota(jnp.int32, (tok, tok), 0)
    col = lax.broadcasted_iota(jnp.int32, (tok, tok), 1)
    tri = jnp.where(col <= row, 1.0, 0.0).astype(f32)
    cum = dot(tri, log_decay, precision=lax.Precision.HIGHEST)
    last = cum[tok - 1 : tok, :]
    kin = (inflow * jnp.exp(last - cum)).astype(bf16)
    through = jnp.exp(last)
    r16 = lax.broadcasted_iota(jnp.int32, (16, HEAD), 0)

    def pack_decay(dec):
        hi = dec.astype(bf16)
        lo = (dec - hi.astype(f32)).astype(bf16)
        zero = jnp.zeros((16, HEAD), f32)
        return jnp.where(
            r16 == 0, hi.astype(f32), jnp.where(r16 == 1, lo.astype(f32), zero)
        ).astype(bf16)

    def unpack_decay(msg):
        rows = msg[HEAD : HEAD + 16, :].astype(f32)
        return rows[0:1] + rows[1:2]

    def unpack_state(msg):
        return msg[0:HEAD, :].astype(f32)

    for h in range(2):
        cols = slice(h * HEAD, (h + 1) * HEAD)
        st = dot(rv[:, cols], kin[:, cols], TN)
        dev_state[h] = st
        dev_decay[h] = through[:, cols]
        sown[h, 0:HEAD, :] = st.astype(bf16)
        sown[h, HEAD : HEAD + 16, :] = pack_decay(through[:, cols])
    send(sown, spart, s_own, st_sem.at[0], partner)
    qe[...] = (rq[...].astype(f32) * jnp.exp(cum)).astype(bf16)

    def local_outputs():
        r64 = lax.broadcasted_iota(jnp.int32, (BLK, BLK), 0)
        c64 = lax.broadcasted_iota(jnp.int32, (BLK, BLK), 1)
        for h in range(2):
            cols = slice(h * HEAD, (h + 1) * HEAD)
            state = None
            for b in range(tok // BLK):
                rows = slice(b * BLK, (b + 1) * BLK)
                blk_cum = cum[rows, cols]
                if b:
                    blk_cum = blk_cum - cum[b * BLK - 1 : b * BLK, cols]
                qd = (rq[rows, cols].astype(f32) * jnp.exp(blk_cum)).astype(bf16)
                kd = (inflow[rows, cols] * jnp.exp(-blk_cum)).astype(bf16)
                scores = dot(qd, kd, NT)
                scores = jnp.where(c64 <= r64, scores, 0.0).astype(bf16)
                res = dot(scores, rv[rows, cols])
                if b:
                    res = res + dot(qd, state.astype(bf16), NT)
                loc[rows, cols] = res
                if b + 1 < tok // BLK:
                    end = blk_cum[BLK - 1 : BLK, :]
                    ke = (inflow[rows, cols] * jnp.exp(end - blk_cum)).astype(bf16)
                    new = dot(rv[rows, cols], ke, TN)
                    state = new if b == 0 else state * jnp.exp(end) + new

    local_outputs()

    got(spart, st_sem.at[0])
    own_s, own_d = dev_state[c], dev_decay[c]
    oth_s, oth_d = unpack_state(spart[c]), unpack_decay(spart[c])
    first_core = c == 0
    late_d = jnp.where(first_core, oth_d, own_d)
    chip_state = late_d * jnp.where(first_core, own_s, oth_s) + jnp.where(first_core, oth_s, own_s)
    tm[0, 0:HEAD, :] = chip_state.astype(bf16)
    tm[0, HEAD : HEAD + 16, :] = pack_decay(own_d * oth_d)

    @pl.when(z + 1 < nz)
    def _():
        send(tm.at[0], tm.at[1], s_tm[0], st_sem.at[1], zdev(1))

    ones = jnp.ones((16, 2 * tok), bf16)

    def pair_update(chip, fresh):
        s0 = chip * 2
        keys = jnp.concatenate([kv[s0, 0], kv[s0 + 1, 0]], axis=0)
        vt = jnp.concatenate(
            [
                kv[s0, 1, 0:HEAD, :], kv[s0, 1, HEAD : 2 * HEAD, :],
                kv[s0 + 1, 1, 0:HEAD, :], kv[s0 + 1, 1, HEAD : 2 * HEAD, :],
            ],
            axis=1,
        )
        vt = jnp.concatenate([vt, ones], axis=0)
        for t in range(4):
            s = dot(keys, qp[t], NT)
            if fresh:
                kpos = lax.broadcasted_iota(jnp.int32, s.shape, 0)
                qpos = lax.broadcasted_iota(jnp.int32, s.shape, 1) + c * tok
                s = jnp.where(kpos <= qpos, s, -1e30)
                new_max = jnp.max(s, axis=0, keepdims=True)
                w = jnp.where(kpos <= qpos, jnp.exp(s - new_max), 0.0).astype(bf16)
                acc[t] = dot(vt, w)
            else:
                old_max = mrow[t]
                new_max = jnp.maximum(old_max, jnp.max(s, axis=0, keepdims=True))
                w = jnp.exp(s - new_max).astype(bf16)
                acc[t] = acc[t] * jnp.exp(old_max - new_max) + dot(vt, w)
            mrow[t] = new_max

    def take_pair(d, i):
        chip = chip_at(d, i)
        slot = chip * 2 + 1 - c
        for kind in range(2):
            got(kv.at[slot, kind], kvp_sem.at[d, 2 * (i - 1) + kind])
        earlier = (z >= i) if d == 0 else (z + i >= nz)

        @pl.when(earlier)
        def _():
            pair_update(chip, False)

    def forward_kv(p):
        i, kind = p // 2 + 1, p % 2
        for d in range(2):

            @pl.when(i <= kv_reach[d])
            def _():
                piece = kv.at[chip_at(d, i) * 2 + c, kind]
                got(piece, kvz_sem.at[d, p])

                @pl.when(i < kv_reach[d])
                def _():
                    send(piece, piece, s_kvz, kvz_sem.at[d, p + 2], ring[d])

                send(piece, piece, s_kvp, kvp_sem.at[d, p], partner)

    def forward_w(p):
        i = p + 1
        for d in range(2):

            @pl.when(i <= w_reach[d])
            def _():
                s = chip_at(d, i) * 2 + c
                piece = wbuf.at[0, s]
                got(piece, wz_sem.at[d, i])

                @pl.when(i < w_reach[d])
                def _():
                    send(piece, piece, s_wz, wz_sem.at[d, i + 1], ring[d])

                send(piece, wbuf.at[3, s], s_wx, wx_sem.at[1, d, i], xdev(1))
                send(piece, wbuf.at[1, s], s_wx, wx_sem.at[0, d, i], xdev(-1))
                send(piece, piece, s_wp, wp_sem.at[0], partner)

        j = p - 1
        for d in range(2):

            @pl.when((j >= d) & (j <= w_reach[d]))
            def _():
                s = chip_at(d, j) * 2 + c
                for k in range(2):
                    rel = 2 * k + 1
                    got(wbuf.at[rel, s], wx_sem.at[k, d, j])
                    send(wbuf.at[rel, s], wbuf.at[rel, s], s_wp, wp_sem.at[0], partner)
                send(wbuf.at[3 - 2 * c, s], wbuf.at[2, s], s_wr, wr_sem.at[d, j], xdev(1 - 2 * c))

        k = p - 3
        for d in range(2):

            @pl.when((k >= d) & (k <= w_reach[d]))
            def _():
                s = chip_at(d, k) * 2 + c
                got(wbuf.at[2, s], wr_sem.at[d, k])
                send(wbuf.at[2, s], wbuf.at[2, s], s_wp, wp_sem.at[0], partner)

    def hand_out(src, which):
        for r in range(1, 4):
            d = (x - r + ntp) % ntp
            rows = src.at[pl.ds(pl.multiple_of(d * rows_out, rows_out), rows_out)]
            send(rows, ract.at[which, r], s_act, act_sem.at[which, r], (g, sp, d))

    turn = 2 * HOPS + 3 * (z // HOPS)

    def state_steps(p):
        @pl.when((p % 2 == 0) & (p >= 2) & (p <= 2 * HOPS))
        def _():
            r = p // 2

            @pl.when(z >= r)
            def _():
                got(tm.at[r], st_sem.at[r])

                @pl.when((r < HOPS) & (z + 1 < nz))
                def _():
                    send(tm.at[r], tm.at[r + 1], send_sem.at[10 + r], st_sem.at[r + 1], zdev(1))

        @pl.when(p == turn)
        def _():
            @pl.when(z >= HOPS)
            def _():
                got(ch.at[0], st_sem.at[HOPS + 1])

            state = unpack_state(ch[0])
            for r in range(HOPS, 0, -1):
                state = state * unpack_decay(tm[r]) + unpack_state(tm[r])
            ch[1, 0:HEAD, :] = state.astype(bf16)

            @pl.when(z + HOPS < nz)
            def _():
                send(ch.at[1], ch.at[0], s_chain, st_sem.at[HOPS + 1], zdev(HOPS))

            send(ch.at[1], pe, s_pe, st_sem.at[HOPS + 2], partner)

        @pl.when(p == turn + 1)
        def _():
            got(pe, st_sem.at[HOPS + 2])
            ours, theirs = unpack_state(ch[1]), unpack_state(pe[...])
            for h in range(2):
                cols = slice(h * HEAD, (h + 1) * HEAD)
                before = jnp.where(c == h, ours, theirs)
                second = before * unpack_decay(spart[h]) + unpack_state(spart[h])
                before = jnp.where(first_core, before, second).astype(bf16)
                mix = loc[:, cols] + dot(qe[:, cols], before, NT)
                mean_square = jnp.mean(mix * mix, axis=-1, keepdims=True)
                arec[:, cols] = (mix * lax.rsqrt(mean_square + EPS) * rgain[...]).astype(bf16)
            hand_out(arec, 0)

    def phase(p, carry):
        forward_kv(p)
        forward_w(p)
        state_steps(p)

        @pl.when(p == 0)
        def _():
            for kind in range(2):
                got(kv.at[z * 2 + 1 - c, kind], kvp_sem.at[0, 2 * half + kind])
            pair_update(z, True)

        i = p // 2
        for d in range(2):

            @pl.when((p >= 2) & (p % 2 == d) & (i <= kv_reach[d]))
            def _():
                take_pair(d, i)

        return carry

    lax.fori_loop(0, 2 * half, phase, 0)
    take_pair(1, half)

    for h in range(2):
        cols = slice(h * HEAD, (h + 1) * HEAD)
        one, two = acc[h], acc[2 + h]
        mix = one[0:HEAD] / one[HEAD : HEAD + 1]
        mix = mix - lam[h : h + 1, 0:1] * (two[0:HEAD] / two[HEAD : HEAD + 1])
        mean_square = jnp.mean(mix * mix, axis=0, keepdims=True)
        mix = jnp.transpose(mix * lax.rsqrt(mean_square + EPS))
        aatt[:, cols] = (mix * again[...]).astype(bf16)
    hand_out(aatt, 1)

    got(wbuf.at[0:4, 0:nz], wp_sem.at[0])
    chunk = 512
    pieces = chunk // 32

    def project(which, src):
        own_rows = src[pl.ds(pl.multiple_of(x * rows_out, rows_out), rows_out), :]
        acts = [own_rows if r == 0 else ract[which, r] for r in range(4)]

        def columns(n):
            total = None
            for r in range(4):
                w = [
                    wbuf[
                        r, pl.ds(n * pieces, pieces),
                        which * 64 + kb * 32 : which * 64 + kb * 32 + 32, :
                    ].reshape(chunk, HEAD)
                    for kb in range(2)
                ]
                term = dot(acts[r], jnp.concatenate(w, axis=1), NT)
                total = term if total is None else total + term
            return total

        return columns

    for r in range(1, 4):
        got(ract.at[0, r], act_sem.at[0, r])
    rec = project(0, arec)
    for n in range(2048 // chunk):
        part[:, n * chunk : (n + 1) * chunk] = rec(n)
    for r in range(1, 4):
        got(ract.at[1, r], act_sem.at[1, r])
    att = project(1, aatt)
    for n in range(2048 // chunk):
        cols = slice(n * chunk, (n + 1) * chunk)
        out[:, cols] = (part[:, cols] + att(n)).astype(bf16)

    got(kv.at[0 : nz - 1], s_kvz)
    got(kv.at[0:nz], s_kvp)
    got(wbuf.at[0, 0 : nz - 1], s_wz)
    got(wbuf.at[0:2, 0:nz], s_wx)
    got(wbuf.at[0, 0:nz], s_wr)
    got(wbuf.at[0:4, 0:nz], s_wp)
    got(sown, s_own)
    got(pe, s_pe)

    @pl.when(z + HOPS < nz)
    def _():
        got(pe, s_chain)

    for r in range(HOPS):

        @pl.when((z + 1 < nz) & (z >= r))
        def _():
            got(pe, s_tm[r])

    got(ract.at[0:2, 1:4], s_act)


def shards(rq, fg, rv, lb, added, rgain, q1, k1, q2, k2, v, lam, again, w, *, nz):
    tok = rq.shape[0]
    half_tok = tok // 2
    keys = jnp.concatenate([k1, k2], axis=1)
    vt = v.reshape(2, half_tok, HEAD).transpose(0, 2, 1).reshape(tok, HEAD)
    kvl = jnp.stack([keys, vt])
    wl = w.reshape(2, 2, HEAD, 32).transpose(0, 1, 3, 2).reshape(HEAD, HEAD)
    scale = jnp.asarray(DA_HD**-0.5, bf16)
    zero = jnp.zeros((tok, DA_HD), bf16)
    qp = jnp.stack(
        [
            jnp.concatenate([q1[:, :DA_HD] * scale, zero], axis=1),
            jnp.concatenate([q1[:, DA_HD:] * scale, zero], axis=1),
            jnp.concatenate([zero, q2[:, :DA_HD] * scale], axis=1),
            jnp.concatenate([zero, q2[:, DA_HD:] * scale], axis=1),
        ]
    )
    vmem = pl.BlockSpec(memory_space=pltpu.VMEM)
    hbm = pl.BlockSpec(memory_space=pltpu.HBM)
    nsp = 2 * nz
    msg = (HEAD + 16, HEAD)
    dma = pltpu.SemaphoreType.DMA
    return pl.pallas_call(
        functools.partial(kernel, nz),
        out_shape=jax.ShapeDtypeStruct((tok // 4, w.shape[2] * nsp), bf16),
        in_specs=[hbm, hbm] + [vmem] * 9,
        out_specs=vmem,
        scratch_shapes=[
            pltpu.VMEM((nsp, 2, tok, HEAD), bf16),
            pltpu.VMEM((4, nsp, HEAD, HEAD), bf16),
            pltpu.VMEM((4, HEAD + 16, tok), f32),
            pltpu.VMEM((4, 1, tok), f32),
            pltpu.VMEM((2,) + msg, bf16),
            pltpu.VMEM((2,) + msg, bf16),
            pltpu.VMEM((HOPS + 1,) + msg, bf16),
            pltpu.VMEM((2,) + msg, bf16),
            pltpu.VMEM(msg, bf16),
            pltpu.VMEM((tok, 2 * HEAD), f32),
            pltpu.VMEM((tok, 2 * HEAD), bf16),
            pltpu.VMEM((2, HEAD, HEAD), f32),
            pltpu.VMEM((2, 1, HEAD), f32),
            pltpu.VMEM((tok, 2 * HEAD), bf16),
            pltpu.VMEM((tok, 2 * HEAD), bf16),
            pltpu.VMEM((2, 4, tok // 4, 2 * HEAD), bf16),
            pltpu.VMEM((tok // 4, w.shape[2] * nsp), f32),
            dma((2,)),
            dma((10 + HOPS,)),
            dma((2, nz + 2)),
            dma((2, nz + 2)),
            dma((2, nz // 2 + 1)),
            dma((2, 2, nz // 2 + 1)),
            dma((2, nz // 2 + 1)),
            dma((1,)),
            dma((HOPS + 3,)),
            dma((2, 4)),
        ],
        compiler_params=pltpu.CompilerParams(
            collective_id=0, has_side_effects=True, vmem_limit_bytes=60 * 1024 * 1024
        ),
    )(
        kvl, wl, qp, rq, fg, rv, lb.reshape(1, -1), added,
        jnp.broadcast_to(lam[:, None], (2, HEAD)), rgain.reshape(1, -1), again.reshape(1, -1),
    )


def solution(mesh):
    tokens = P(("grp", "sp"), "tp")
    return jax.shard_map(
        functools.partial(shards, nz=mesh.shape["sp"] // 2),
        mesh=mesh,
        in_specs=(
            tokens, tokens, tokens, P("tp"), tokens, P(),
            tokens, tokens, tokens, tokens, tokens, P("tp"), P(), P(None, "tp", "sp"),
        ),
        out_specs=P(("grp", "sp", "tp"), None),
        check_vma=False,
    )
```

```python
import functools

import jax
import jax.numpy as jnp
from jax import lax
from jax.experimental import pallas as pl
from jax.experimental.pallas import tpu as pltpu
from jax.sharding import PartitionSpec as P

HEAD = 128
DA_HD = 64
BLK = 64
HOPS = 4
EPS = 1e-06
f32, bf16 = jnp.float32, jnp.bfloat16
NT = (((1,), (1,)), ((), ()))
TN = (((0,), (0,)), ((), ()))


def dot(a, b, dims=(((1,), (0,)), ((), ())), precision=None):
    return lax.dot_general(a, b, dims, precision=precision, preferred_element_type=f32)


def kernel(
    nz, kvl, wl, qp, rq, fg, rv, lb, added, lam, rgain, again, out,
    kv, wbuf, acc, mrow, sown, spart, tm, ch, pe, loc, qe, dev_state, dev_decay,
    arec, aatt, ract, part,
    copy_sem, send_sem, skz_sem, skp_sem, kvz_sem, kvp_sem, kvo_sem, wz_sem, wx_sem, wr_sem,
    wp_sem, st_sem, act_sem, chain_ready, wrap_ready,
):
    g, sp, x = lax.axis_index("grp"), lax.axis_index("sp"), lax.axis_index("tp")
    ntp = lax.axis_size("tp")
    z, c = sp // 2, sp % 2
    up = c == 0
    top = nz - 1
    half = nz // 2
    kv_up = (5 * nz) // 8
    kv_wrap = nz - 1 - kv_up
    w_far = (half, half - 1)
    gap = jnp.maximum(half // 2 + 1 - z, 0)
    meet = 10
    tok = rq.shape[0]
    rows_out = tok // ntp
    mesh_id = pl.DeviceIdType.MESH

    def zdev(chip):
        return (g, chip * 2 + c, x)

    def xdev(dx):
        return (g, sp, (x + dx + ntp) % ntp)

    partner = (g, z * 2 + 1 - c, x)
    ring = (zdev((z + 1) % nz), zdev((z - 1 + nz) % nz))

    def send(src, dst, s_sem, r_sem, to):
        pltpu.make_async_remote_copy(
            src_ref=src, dst_ref=dst, send_sem=s_sem, recv_sem=r_sem,
            device_id=to, device_id_type=mesh_id,
        ).start()

    def got(ref, sem):
        pltpu.make_async_copy(ref, ref, sem).wait()

    def tell(sem, dev):
        pl.semaphore_signal(sem, inc=1, device_id=dev, device_id_type=mesh_id)

    def chip_from(d, i):
        return (z - i + nz) % nz if d == 0 else (z + i) % nz

    def item(d, u):
        if d == 1:
            return u
        return jnp.where(u <= z, u, jnp.where(u > z + gap, u - gap, -1))

    def kv_used(d, i):
        if d == 0:
            return (i >= 1) & (i <= kv_up) & (z >= i)
        return (i >= 1) & (i <= kv_wrap) & (z + i >= nz)

    def kv_in(d, i):
        if d == 0:
            return kv_used(0, i)
        return kv_used(1, i) | (i >= 1) & (z + i < kv_wrap)

    def kv_out(d, i):
        own = z < (top if d == 0 else kv_wrap)
        on = (z < top) & (i < kv_up) if d == 0 else i < kv_wrap
        return (i == 0) & own | kv_in(d, i) & on

    def kv_pair(kind, chip):
        return kv.at[kind, pl.ds(2 * chip, 2)]

    loads = [pltpu.make_async_copy(kvl.at[k], kv.at[k, sp], copy_sem.at[k]) for k in range(2)]
    loads.append(pltpu.make_async_copy(wl, wbuf.at[0, sp], copy_sem.at[2]))
    for load in loads:
        load.start()
    tm[...] = jnp.zeros_like(tm)
    ch[...] = jnp.zeros_like(ch)

    barrier = pltpu.get_barrier_semaphore()

    def greet(cond, dev):
        @pl.when(cond)
        def _():
            tell(barrier, dev)

    for dx in range(1, 4):
        tell(barrier, xdev(dx))
    tell(barrier, partner)
    greet(z < top, zdev(jnp.minimum(z + 1, top)))
    greet(z > 0, zdev(jnp.maximum(z - 1, 0)))
    greet(z + HOPS <= top, zdev(jnp.minimum(z + HOPS, top)))
    greet(z == 0, zdev(top))
    one = jnp.int32(1)
    none = jnp.int32(0)
    callers = 4 + jnp.where(z < top, one, none) + jnp.where(z > 0, one, none)
    callers = callers + jnp.where(z >= HOPS, one, none)
    callers = callers + jnp.where(z == top, one, none)
    pl.semaphore_wait(barrier, callers)

    @pl.when(z >= HOPS)
    def _():
        tell(chain_ready, zdev(jnp.maximum(z - HOPS, 0)))

    @pl.when(z == top)
    def _():
        tell(wrap_ready, zdev(0))

    s_wz, s_wx, s_wr, s_wp, s_act, s_own, s_chain, s_pe = (send_sem.at[k] for k in range(8))
    s_tm = [send_sem.at[9 + r] for r in range(HOPS)]
    s_kvo = [send_sem.at[9 + HOPS + k] for k in range(2)]

    def send_kv(d, i, kind):
        piece = kv.at[kind, chip_from(d, i) * 2 + c]
        send(piece, piece, skz_sem.at[d, i, kind], kvz_sem.at[d, i + 1, kind], ring[d])

    def send_w(d, i):
        piece = wbuf.at[0, chip_from(d, i) * 2 + c]
        send(piece, piece, s_wz, wz_sem.at[d, i + 1], ring[d])

    loads[0].wait()
    loads[1].wait()
    for kind in range(2):
        for d in range(2):

            @pl.when(kv_out(d, 0) & ((z > 0) | (d == 0)))
            def _():
                send_kv(d, jnp.int32(0), kind)

        mine = kv.at[kind, sp]
        send(mine, mine, s_kvo[kind], kvo_sem.at[kind], partner)
    loads[2].wait()
    mine = wbuf.at[0, sp]
    send_w(0, jnp.int32(0))

    @pl.when(z > 0)
    def _():
        send_w(1, jnp.int32(0))

    send(mine, mine, s_wp, wp_sem.at[0], partner)
    send(mine, wbuf.at[3, sp], s_wx, wx_sem.at[1, 0, 0], xdev(1))
    send(mine, wbuf.at[1, sp], s_wx, wx_sem.at[0, 0, 0], xdev(-1))

    floor_rate = jax.nn.sigmoid(-lb[...])
    inflow = floor_rate * jax.nn.sigmoid(-fg[...].astype(f32))
    one_less = 1.0 - inflow
    add2 = added[...]
    add_wide = jnp.concatenate(
        [jnp.broadcast_to(add2[:, h : h + 1], (tok, HEAD)) for h in range(2)], axis=1
    )
    log_decay = jnp.log(one_less) - ((one_less - 1.0) + inflow) / one_less + add_wide
    row = lax.broadcasted_iota(jnp.int32, (tok, tok), 0)
    col = lax.broadcasted_iota(jnp.int32, (tok, tok), 1)
    tri = jnp.where(col <= row, 1.0, 0.0).astype(f32)
    cum = dot(tri, log_decay, precision=lax.Precision.HIGHEST)
    last = cum[tok - 1 : tok, :]
    kin = (inflow * jnp.exp(last - cum)).astype(bf16)
    through = jnp.exp(last)
    r16 = lax.broadcasted_iota(jnp.int32, (16, HEAD), 0)

    def pack_decay(dec):
        hi = dec.astype(bf16)
        lo = (dec - hi.astype(f32)).astype(bf16)
        zero = jnp.zeros((16, HEAD), f32)
        return jnp.where(
            r16 == 0, hi.astype(f32), jnp.where(r16 == 1, lo.astype(f32), zero)
        ).astype(bf16)

    def unpack_decay(msg):
        rows = msg[HEAD : HEAD + 16, :].astype(f32)
        return rows[0:1] + rows[1:2]

    def unpack_state(msg):
        return msg[0:HEAD, :].astype(f32)

    for h in range(2):
        cols = slice(h * HEAD, (h + 1) * HEAD)
        st = dot(rv[:, cols], kin[:, cols], TN)
        dev_state[h] = st
        dev_decay[h] = through[:, cols]
        sown[h, 0:HEAD, :] = st.astype(bf16)
        sown[h, HEAD : HEAD + 16, :] = pack_decay(through[:, cols])
    send(sown, spart, s_own, st_sem.at[0], partner)

    got(spart, st_sem.at[0])
    own_s, own_d = dev_state[c], dev_decay[c]
    oth_s, oth_d = unpack_state(spart[c]), unpack_decay(spart[c])
    late_d = jnp.where(up, oth_d, own_d)
    chip_state = late_d * jnp.where(up, own_s, oth_s) + jnp.where(up, oth_s, own_s)
    tm[0, 0:HEAD, :] = chip_state.astype(bf16)
    tm[0, HEAD : HEAD + 16, :] = pack_decay(own_d * oth_d)
    above = zdev(jnp.minimum(z + 1, top))

    @pl.when(z < top)
    def _():
        send(tm.at[0], tm.at[1], s_tm[0], st_sem.at[1], above)

    qe[...] = (rq[...].astype(f32) * jnp.exp(cum)).astype(bf16)

    def local_outputs():
        r64 = lax.broadcasted_iota(jnp.int32, (BLK, BLK), 0)
        c64 = lax.broadcasted_iota(jnp.int32, (BLK, BLK), 1)
        for h in range(2):
            cols = slice(h * HEAD, (h + 1) * HEAD)
            state = None
            for b in range(tok // BLK):
                rows = slice(b * BLK, (b + 1) * BLK)
                blk_cum = cum[rows, cols]
                if b:
                    blk_cum = blk_cum - cum[b * BLK - 1 : b * BLK, cols]
                qd = (rq[rows, cols].astype(f32) * jnp.exp(blk_cum)).astype(bf16)
                kd = (inflow[rows, cols] * jnp.exp(-blk_cum)).astype(bf16)
                scores = dot(qd, kd, NT)
                scores = jnp.where(c64 <= r64, scores, 0.0).astype(bf16)
                res = dot(scores, rv[rows, cols])
                if b:
                    res = res + dot(qd, state.astype(bf16), NT)
                loc[rows, cols] = res
                if b + 1 < tok // BLK:
                    end = blk_cum[BLK - 1 : BLK, :]
                    ke = (inflow[rows, cols] * jnp.exp(end - blk_cum)).astype(bf16)
                    new = dot(rv[rows, cols], ke, TN)
                    state = new if b == 0 else state * jnp.exp(end) + new

    ones = jnp.ones((16, 2 * tok), bf16)

    def pair_update(chip, fresh):
        s0 = chip * 2
        keys = kv[0, pl.ds(s0, 2)].reshape(2 * tok, HEAD)
        vt = jnp.concatenate(
            [
                kv[1, s0, 0:HEAD, :], kv[1, s0, HEAD : 2 * HEAD, :],
                kv[1, s0 + 1, 0:HEAD, :], kv[1, s0 + 1, HEAD : 2 * HEAD, :],
            ],
            axis=1,
        )
        vt = jnp.concatenate([vt, ones], axis=0)
        scores = [dot(keys, qp[t], NT) for t in range(4)]
        for t in range(4):
            s = scores[t]
            if fresh:
                kpos = lax.broadcasted_iota(jnp.int32, s.shape, 0)
                qpos = lax.broadcasted_iota(jnp.int32, s.shape, 1) + c * tok
                s = jnp.where(kpos <= qpos, s, -1e30)
                new_max = jnp.max(s, axis=0, keepdims=True)
                w = jnp.where(kpos <= qpos, jnp.exp(s - new_max), 0.0).astype(bf16)
                acc[t] = dot(vt, w)
            else:
                old_max = mrow[t]
                new_max = jnp.maximum(old_max, jnp.max(s, axis=0, keepdims=True))
                w = jnp.exp(s - new_max).astype(bf16)
                acc[t] = acc[t] * jnp.exp(old_max - new_max) + dot(vt, w)
            mrow[t] = new_max

    def forward_w(d, u):
        i = item(d, u)

        @pl.when((i >= 1) & (i <= w_far[d]))
        def _():
            s = chip_from(d, i) * 2 + c
            piece = wbuf.at[0, s]
            got(piece, wz_sem.at[d, i])

            @pl.when((i < w_far[d]) & ((z > 0) | (u >= meet) | (d == 0)))
            def _():
                send_w(d, i)

            send(piece, wbuf.at[3, s], s_wx, wx_sem.at[1, d, i], xdev(1))
            send(piece, wbuf.at[1, s], s_wx, wx_sem.at[0, d, i], xdev(-1))
            send(piece, piece, s_wp, wp_sem.at[0], partner)

    def spread_w(d, u):
        j = item(d, u - 2)

        @pl.when((j >= d) & (j <= w_far[d]) & (u >= 2))
        def _():
            s = chip_from(d, j) * 2 + c
            for k in range(2):
                ref = wbuf.at[2 * k + 1, s]
                got(ref, wx_sem.at[k, d, j])
                send(ref, ref, s_wp, wp_sem.at[0], partner)
            send(wbuf.at[3 - 2 * c, s], wbuf.at[2, s], s_wr, wr_sem.at[d, j], xdev(1 - 2 * c))

        q = item(d, u - 4)

        @pl.when((q >= d) & (q <= w_far[d]) & (u >= 4))
        def _():
            ref = wbuf.at[2, chip_from(d, q) * 2 + c]
            got(ref, wr_sem.at[d, q])
            send(ref, ref, s_wp, wp_sem.at[0], partner)

    def forward_kv(d, u, kind):
        i = item(d, u)

        @pl.when(kv_in(d, i))
        def _():
            piece = kv.at[kind, chip_from(d, i) * 2 + c]
            got(piece, kvz_sem.at[d, i, kind])

            @pl.when(kv_out(d, i) & ((z > 0) | (u >= meet) | (d == 0)))
            def _():
                send_kv(d, i, kind)

            @pl.when(kv_used(d, i))
            def _():
                send(piece, piece, skp_sem.at[d, i, kind], kvp_sem.at[d, i, kind], partner)

    def take(d, u):
        i = item(d, u - 1)

        @pl.when(kv_used(d, i) & (u >= 1))
        def _():
            chip = chip_from(d, i)
            for kind in range(2):
                got(kv.at[kind, chip * 2 + 1 - c], kvp_sem.at[d, i, kind])
            pair_update(chip, False)

    def meet_top(u):
        @pl.when((z == 0) & (u == meet))
        def _():
            pl.semaphore_wait(wrap_ready, 1)

            def late(k, carry):
                send_w(1, k)
                for kind in range(2):

                    @pl.when(kv_out(1, k))
                    def _():
                        send_kv(1, k, kind)

                return carry

            lax.fori_loop(0, meet, late, 0)

    def hand_out(src, which):
        for r in range(1, 4):
            d = (x - r + ntp) % ntp
            rows = src.at[pl.ds(pl.multiple_of(d * rows_out, rows_out), rows_out)]
            send(rows, ract.at[which, r], s_act, act_sem.at[which, r], (g, sp, d))

    late_turn = jnp.maximum((z - 3 * HOPS) // HOPS, 0)
    turn = HOPS + 1 + late_turn

    def state_steps(i):
        @pl.when((i >= 1) & (i <= HOPS) & (z >= i))
        def _():
            got(tm.at[i], st_sem.at[i])

            @pl.when((i < HOPS) & (z < top))
            def _():
                send(tm.at[i], tm.at[i + 1], send_sem.at[9 + i], st_sem.at[i + 1], above)

        @pl.when(i == turn)
        def _():
            @pl.when(z >= HOPS)
            def _():
                got(ch.at[0], st_sem.at[HOPS + 1])

            state = unpack_state(ch[0])
            for r in range(HOPS, 0, -1):
                state = state * unpack_decay(tm[r]) + unpack_state(tm[r])
            ch[1, 0:HEAD, :] = state.astype(bf16)
            send(ch.at[1], pe, s_pe, st_sem.at[HOPS + 2], partner)

            @pl.when(z + HOPS <= top)
            def _():
                pl.semaphore_wait(chain_ready, 1)
                send(
                    ch.at[1], ch.at[0], s_chain, st_sem.at[HOPS + 1],
                    zdev(jnp.minimum(z + HOPS, top)),
                )

        @pl.when(i == turn + 1)
        def _():
            got(pe, st_sem.at[HOPS + 2])
            ours, theirs = unpack_state(ch[1]), unpack_state(pe[...])
            for h in range(2):
                cols = slice(h * HEAD, (h + 1) * HEAD)
                before = jnp.where(c == h, ours, theirs)
                second = before * unpack_decay(spart[h]) + unpack_state(spart[h])
                before = jnp.where(up, before, second).astype(bf16)
                mix = loc[:, cols] + dot(qe[:, cols], before, NT)
                mean_square = jnp.mean(mix * mix, axis=-1, keepdims=True)
                arec[:, cols] = (mix * lax.rsqrt(mean_square + EPS) * rgain[...]).astype(bf16)
            hand_out(arec, 0)

    def step(u, carry):
        meet_top(u)
        for d in range(2):
            forward_w(d, u)
        for d in range(2):
            forward_kv(d, u, 0)
        state_steps(u)
        take(0, u)
        for d in range(2):
            forward_kv(d, u, 1)
        for d in range(2):
            spread_w(d, u)
        take(1, u)

        @pl.when(u == 0)
        def _():
            local_outputs()
            for kind in range(2):
                got(kv.at[kind, z * 2 + 1 - c], kvo_sem.at[kind])
            pair_update(z, True)

        return carry

    lax.fori_loop(0, half + half // 2 + 7, step, 0)

    for h in range(2):
        cols = slice(h * HEAD, (h + 1) * HEAD)
        first, second = acc[h], acc[2 + h]
        mix = first[0:HEAD] / first[HEAD : HEAD + 1]
        mix = mix - lam[h : h + 1, 0:1] * (second[0:HEAD] / second[HEAD : HEAD + 1])
        mean_square = jnp.mean(mix * mix, axis=0, keepdims=True)
        mix = jnp.transpose(mix * lax.rsqrt(mean_square + EPS))
        aatt[:, cols] = (mix * again[...]).astype(bf16)
    hand_out(aatt, 1)

    got(wbuf.at[0:4, 0:nz], wp_sem.at[0])
    chunk = 512
    pieces = chunk // 32

    def project(which, src):
        own_rows = src[pl.ds(pl.multiple_of(x * rows_out, rows_out), rows_out), :]
        acts = [own_rows if r == 0 else ract[which, r] for r in range(4)]

        def columns(n):
            total = None
            for r in range(4):
                w = [
                    wbuf[
                        r, pl.ds(n * pieces, pieces),
                        which * 64 + kb * 32 : which * 64 + kb * 32 + 32, :
                    ].reshape(chunk, HEAD)
                    for kb in range(2)
                ]
                term = dot(acts[r], jnp.concatenate(w, axis=1), NT)
                total = term if total is None else total + term
            return total

        return columns

    for r in range(1, 4):
        got(ract.at[0, r], act_sem.at[0, r])
    rec = project(0, arec)
    for n in range(2048 // chunk):
        part[:, n * chunk : (n + 1) * chunk] = rec(n)
    for r in range(1, 4):
        got(ract.at[1, r], act_sem.at[1, r])
    att = project(1, aatt)
    for n in range(2048 // chunk):
        cols = slice(n * chunk, (n + 1) * chunk)
        out[:, cols] = (part[:, cols] + att(n)).astype(bf16)

    def drain(i, carry):
        for d in range(2):
            for kind in range(2):

                @pl.when(kv_out(d, i))
                def _():
                    got(kv.at[kind, 0], skz_sem.at[d, i, kind])

                @pl.when(kv_used(d, i))
                def _():
                    got(kv.at[kind, 0], skp_sem.at[d, i, kind])

        return carry

    lax.fori_loop(0, kv_up + 1, drain, 0)
    for kind in range(2):
        got(kv.at[kind, 0], s_kvo[kind])
    got(wbuf.at[0, 0 : nz - 1], s_wz)
    got(wbuf.at[0:2, 0:nz], s_wx)
    got(wbuf.at[0, 0:nz], s_wr)
    got(wbuf.at[0:4, 0:nz], s_wp)
    got(sown, s_own)
    got(pe, s_pe)

    @pl.when(z + HOPS <= top)
    def _():
        got(pe, s_chain)

    for r in range(HOPS):

        @pl.when((z < top) & (z >= r))
        def _():
            got(pe, s_tm[r])

    got(ract.at[0:2, 1:4], s_act)


def shards(rq, fg, rv, lb, added, rgain, q1, k1, q2, k2, v, lam, again, w, *, nz):
    tok = rq.shape[0]
    half_tok = tok // 2
    keys = jnp.concatenate([k1, k2], axis=1)
    vt = v.reshape(2, half_tok, HEAD).transpose(0, 2, 1).reshape(tok, HEAD)
    kvl = jnp.stack([keys, vt])
    wl = w.reshape(2, 2, HEAD, 32).transpose(0, 1, 3, 2).reshape(HEAD, HEAD)
    scale = jnp.asarray(DA_HD**-0.5, bf16)
    zero = jnp.zeros((tok, DA_HD), bf16)
    qp = jnp.stack(
        [
            jnp.concatenate([q1[:, :DA_HD] * scale, zero], axis=1),
            jnp.concatenate([q1[:, DA_HD:] * scale, zero], axis=1),
            jnp.concatenate([zero, q2[:, :DA_HD] * scale], axis=1),
            jnp.concatenate([zero, q2[:, DA_HD:] * scale], axis=1),
        ]
    )
    vmem = pl.BlockSpec(memory_space=pltpu.VMEM)
    hbm = pl.BlockSpec(memory_space=pltpu.HBM)
    nsp = 2 * nz
    msg = (HEAD + 16, HEAD)
    dma = pltpu.SemaphoreType.DMA
    return pl.pallas_call(
        functools.partial(kernel, nz),
        out_shape=jax.ShapeDtypeStruct((tok // 4, w.shape[2] * nsp), bf16),
        in_specs=[hbm, hbm] + [vmem] * 9,
        out_specs=vmem,
        scratch_shapes=[
            pltpu.VMEM((2, nsp, tok, HEAD), bf16),
            pltpu.VMEM((4, nsp, HEAD, HEAD), bf16),
            pltpu.VMEM((4, HEAD + 16, tok), f32),
            pltpu.VMEM((4, 1, tok), f32),
            pltpu.VMEM((2,) + msg, bf16),
            pltpu.VMEM((2,) + msg, bf16),
            pltpu.VMEM((HOPS + 1,) + msg, bf16),
            pltpu.VMEM((2,) + msg, bf16),
            pltpu.VMEM(msg, bf16),
            pltpu.VMEM((tok, 2 * HEAD), f32),
            pltpu.VMEM((tok, 2 * HEAD), bf16),
            pltpu.VMEM((2, HEAD, HEAD), f32),
            pltpu.VMEM((2, 1, HEAD), f32),
            pltpu.VMEM((tok, 2 * HEAD), bf16),
            pltpu.VMEM((tok, 2 * HEAD), bf16),
            pltpu.VMEM((2, 4, tok // 4, 2 * HEAD), bf16),
            pltpu.VMEM((tok // 4, w.shape[2] * nsp), f32),
            dma((3,)),
            dma((11 + HOPS,)),
            dma((2, (5 * nz) // 8 + 2, 2)),
            dma((2, (5 * nz) // 8 + 2, 2)),
            dma((2, (5 * nz) // 8 + 2, 2)),
            dma((2, (5 * nz) // 8 + 2, 2)),
            dma((2,)),
            dma((2, nz // 2 + 2)),
            dma((2, 2, nz // 2 + 1)),
            dma((2, nz // 2 + 1)),
            dma((1,)),
            dma((HOPS + 3,)),
            dma((2, 4)),
            pltpu.SemaphoreType.REGULAR,
            pltpu.SemaphoreType.REGULAR,
        ],
        compiler_params=pltpu.CompilerParams(
            collective_id=0, has_side_effects=True, vmem_limit_bytes=60 * 1024 * 1024
        ),
    )(
        kvl, wl, qp, rq, fg, rv, lb.reshape(1, -1), added,
        jnp.broadcast_to(lam[:, None], (2, HEAD)), rgain.reshape(1, -1), again.reshape(1, -1),
    )


def solution(mesh):
    tokens = P(("grp", "sp"), "tp")
    return jax.shard_map(
        functools.partial(shards, nz=mesh.shape["sp"] // 2),
        mesh=mesh,
        in_specs=(
            tokens, tokens, tokens, P("tp"), tokens, P(),
            tokens, tokens, tokens, tokens, tokens, P("tp"), P(), P(None, "tp", "sp"),
        ),
        out_specs=P(("grp", "sp", "tp"), None),
        check_vma=False,
    )
```

```python
import functools

import jax
import jax.numpy as jnp
from jax import lax
from jax.experimental import pallas as pl
from jax.experimental.pallas import tpu as pltpu
from jax.sharding import PartitionSpec as P

HEAD = 128
DA_HD = 64
BLK = 64
HOPS = 4
EPS = 1e-06
f32, bf16 = jnp.float32, jnp.bfloat16
NT = (((1,), (1,)), ((), ()))
TN = (((0,), (0,)), ((), ()))


def dot(a, b, dims=(((1,), (0,)), ((), ())), precision=None):
    return lax.dot_general(a, b, dims, precision=precision, preferred_element_type=f32)


def kernel(
    nz, kvl, wl, qp_in, rq_in, fg_in, rv_in, lb, added, lam, rgain, again, out,
    qp, rq, fg, rv,
    kv, wbuf, acc, mrow, sown, spart, tm, ch, pe, loc, qe, dev_state, dev_decay,
    arec, aatt, ract, part,
    copy_sem, send_sem, skz_sem, skp_sem, kvz_sem, kvp_sem, kvo_sem, wz_sem, wx_sem, wr_sem,
    wp_sem, st_sem, act_sem, chain_ready, wrap_ready,
):
    g, sp, x = lax.axis_index("grp"), lax.axis_index("sp"), lax.axis_index("tp")
    ntp = lax.axis_size("tp")
    z, c = sp // 2, sp % 2
    up = c == 0
    top = nz - 1
    half = nz // 2
    kv_up = (21 * nz) // 32
    kv_wrap = nz - 1 - kv_up
    w_far = (half, half - 1)
    gap = jnp.maximum(1 - z, 0)
    meet = 1
    tok = rq.shape[0]
    rows_out = tok // ntp
    mesh_id = pl.DeviceIdType.MESH

    def zdev(chip):
        return (g, chip * 2 + c, x)

    def xdev(dx):
        return (g, sp, (x + dx + ntp) % ntp)

    partner = (g, z * 2 + 1 - c, x)
    ring = (zdev((z + 1) % nz), zdev((z - 1 + nz) % nz))

    def send(src, dst, s_sem, r_sem, to):
        pltpu.make_async_remote_copy(
            src_ref=src, dst_ref=dst, send_sem=s_sem, recv_sem=r_sem,
            device_id=to, device_id_type=mesh_id,
        ).start()

    def got(ref, sem):
        pltpu.make_async_copy(ref, ref, sem).wait()

    def tell(sem, dev):
        pl.semaphore_signal(sem, inc=1, device_id=dev, device_id_type=mesh_id)

    def chip_from(d, i):
        return (z - i + nz) % nz if d == 0 else (z + i) % nz

    def item(d, u):
        if d == 1:
            return u
        return jnp.where(u <= z, u, jnp.where(u > z + gap, u - gap, -1))

    def w_item(d, u, v):
        if d == 1:
            return u if v == 0 else jnp.int32(-1)
        low = item(0, u) if v == 0 else jnp.int32(-1)
        low = jnp.where(u > z + gap, z + 2 * (u - z - gap) - 1 + v, low)
        near = z - half
        steps = (near + 1) // 2
        fast = jnp.where((u >= 1) & (2 * u - 1 + v <= near), 2 * u - 1 + v, u if v == 0 else -1)
        fast = jnp.where((u >= 1) & (v == 1) & (2 * u > near), -1, fast)
        slow = near + u - steps if v == 0 else jnp.int32(-1)
        high = jnp.where(u <= steps, fast, slow)
        return jnp.where(z < half, low, high)

    def kv_used(d, i):
        if d == 0:
            return (i >= 1) & (i <= kv_up) & (z >= i)
        return (i >= 1) & (i <= kv_wrap) & (z + i >= nz)

    def kv_in(d, i):
        if d == 0:
            return kv_used(0, i)
        return kv_used(1, i) | (i >= 1) & (z + i < kv_wrap)

    def kv_out(d, i):
        own = z < (top if d == 0 else kv_wrap)
        on = (z < top) & (i < kv_up) if d == 0 else i < kv_wrap
        return (i == 0) & own | kv_in(d, i) & on

    def kv_pair(kind, chip):
        return kv.at[kind, pl.ds(2 * chip, 2)]

    loads = [pltpu.make_async_copy(kvl.at[k], kv.at[k, sp], copy_sem.at[k]) for k in range(2)]
    loads.append(pltpu.make_async_copy(wl, wbuf.at[0, sp], copy_sem.at[2]))
    for k, (src, dst) in enumerate(((fg_in, fg), (rv_in, rv), (rq_in, rq), (qp_in, qp))):
        loads.append(pltpu.make_async_copy(src, dst, copy_sem.at[3 + k]))
    for load in loads:
        load.start()
    tm[...] = jnp.zeros_like(tm)
    ch[...] = jnp.zeros_like(ch)

    barrier = pltpu.get_barrier_semaphore()

    def greet(cond, dev):
        @pl.when(cond)
        def _():
            tell(barrier, dev)

    for dx in range(1, 4):
        tell(barrier, xdev(dx))
    tell(barrier, partner)
    greet(z < top, zdev(jnp.minimum(z + 1, top)))
    greet(z > 0, zdev(jnp.maximum(z - 1, 0)))
    greet(z + HOPS <= top, zdev(jnp.minimum(z + HOPS, top)))
    greet(z == 0, zdev(top))
    one = jnp.int32(1)
    none = jnp.int32(0)
    callers = 4 + jnp.where(z < top, one, none) + jnp.where(z > 0, one, none)
    callers = callers + jnp.where(z >= HOPS, one, none)
    callers = callers + jnp.where(z == top, one, none)
    pl.semaphore_wait(barrier, callers)

    @pl.when(z >= HOPS)
    def _():
        tell(chain_ready, zdev(jnp.maximum(z - HOPS, 0)))

    @pl.when(z == top)
    def _():
        tell(wrap_ready, zdev(0))

    s_wz, s_wx, s_wr, s_wp, s_act, s_own, s_chain, s_pe = (send_sem.at[k] for k in range(8))
    s_tm = [send_sem.at[9 + r] for r in range(HOPS)]
    s_kvo = [send_sem.at[9 + HOPS + k] for k in range(2)]

    def send_kv(d, i, kind):
        piece = kv.at[kind, chip_from(d, i) * 2 + c]
        send(piece, piece, skz_sem.at[d, i, kind], kvz_sem.at[d, i + 1, kind], ring[d])

    def send_w(d, i):
        piece = wbuf.at[0, chip_from(d, i) * 2 + c]
        send(piece, piece, s_wz, wz_sem.at[d, i + 1], ring[d])

    loads[0].wait()
    loads[1].wait()
    for kind in range(2):
        for d in range(2):

            @pl.when(kv_out(d, 0) & ((z > 0) | (d == 0)))
            def _():
                send_kv(d, jnp.int32(0), kind)

        mine = kv.at[kind, sp]
        send(mine, mine, s_kvo[kind], kvo_sem.at[kind], partner)
    loads[2].wait()
    mine = wbuf.at[0, sp]
    send_w(0, jnp.int32(0))

    @pl.when(z > 0)
    def _():
        send_w(1, jnp.int32(0))

    send(mine, mine, s_wp, wp_sem.at[0], partner)
    send(mine, wbuf.at[3, sp], s_wx, wx_sem.at[1, 0, 0], xdev(1))
    send(mine, wbuf.at[1, sp], s_wx, wx_sem.at[0, 0, 0], xdev(-1))

    for load in loads[3:]:
        load.wait()
    floor_rate = jax.nn.sigmoid(-lb[...])
    inflow = floor_rate * jax.nn.sigmoid(-fg[...].astype(f32))
    one_less = 1.0 - inflow
    add2 = added[...]
    add_wide = jnp.concatenate(
        [jnp.broadcast_to(add2[:, h : h + 1], (tok, HEAD)) for h in range(2)], axis=1
    )
    log_decay = jnp.log(one_less) - ((one_less - 1.0) + inflow) / one_less + add_wide
    row = lax.broadcasted_iota(jnp.int32, (tok, tok), 0)
    col = lax.broadcasted_iota(jnp.int32, (tok, tok), 1)
    tri = jnp.where(col <= row, 1.0, 0.0).astype(f32)
    cum = dot(tri, log_decay, precision=lax.Precision.HIGHEST)
    last = cum[tok - 1 : tok, :]
    kin = (inflow * jnp.exp(last - cum)).astype(bf16)
    through = jnp.exp(last)
    r16 = lax.broadcasted_iota(jnp.int32, (16, HEAD), 0)

    def pack_decay(dec):
        hi = dec.astype(bf16)
        lo = (dec - hi.astype(f32)).astype(bf16)
        zero = jnp.zeros((16, HEAD), f32)
        return jnp.where(
            r16 == 0, hi.astype(f32), jnp.where(r16 == 1, lo.astype(f32), zero)
        ).astype(bf16)

    def unpack_decay(msg):
        rows = msg[HEAD : HEAD + 16, :].astype(f32)
        return rows[0:1] + rows[1:2]

    def unpack_state(msg):
        return msg[0:HEAD, :].astype(f32)

    for h in range(2):
        cols = slice(h * HEAD, (h + 1) * HEAD)
        st = dot(rv[:, cols], kin[:, cols], TN)
        dev_state[h] = st
        dev_decay[h] = through[:, cols]
        sown[h, 0:HEAD, :] = st.astype(bf16)
        sown[h, HEAD : HEAD + 16, :] = pack_decay(through[:, cols])
    send(sown, spart, s_own, st_sem.at[0], partner)

    got(spart, st_sem.at[0])
    own_s, own_d = dev_state[c], dev_decay[c]
    oth_s, oth_d = unpack_state(spart[c]), unpack_decay(spart[c])
    late_d = jnp.where(up, oth_d, own_d)
    chip_state = late_d * jnp.where(up, own_s, oth_s) + jnp.where(up, oth_s, own_s)
    tm[0, 0:HEAD, :] = chip_state.astype(bf16)
    tm[0, HEAD : HEAD + 16, :] = pack_decay(own_d * oth_d)
    above = zdev(jnp.minimum(z + 1, top))

    @pl.when(z < top)
    def _():
        send(tm.at[0], tm.at[1], s_tm[0], st_sem.at[1], above)

    qe[...] = (rq[...].astype(f32) * jnp.exp(cum)).astype(bf16)

    def local_outputs():
        r64 = lax.broadcasted_iota(jnp.int32, (BLK, BLK), 0)
        c64 = lax.broadcasted_iota(jnp.int32, (BLK, BLK), 1)
        for h in range(2):
            cols = slice(h * HEAD, (h + 1) * HEAD)
            state = None
            for b in range(tok // BLK):
                rows = slice(b * BLK, (b + 1) * BLK)
                blk_cum = cum[rows, cols]
                if b:
                    blk_cum = blk_cum - cum[b * BLK - 1 : b * BLK, cols]
                qd = (rq[rows, cols].astype(f32) * jnp.exp(blk_cum)).astype(bf16)
                kd = (inflow[rows, cols] * jnp.exp(-blk_cum)).astype(bf16)
                scores = dot(qd, kd, NT)
                scores = jnp.where(c64 <= r64, scores, 0.0).astype(bf16)
                res = dot(scores, rv[rows, cols])
                if b:
                    res = res + dot(qd, state.astype(bf16), NT)
                loc[rows, cols] = res
                if b + 1 < tok // BLK:
                    end = blk_cum[BLK - 1 : BLK, :]
                    ke = (inflow[rows, cols] * jnp.exp(end - blk_cum)).astype(bf16)
                    new = dot(rv[rows, cols], ke, TN)
                    state = new if b == 0 else state * jnp.exp(end) + new

    ones = jnp.ones((16, 2 * tok), bf16)

    def pair_update(chip, fresh):
        s0 = chip * 2
        keys = kv[0, pl.ds(s0, 2)].reshape(2 * tok, HEAD)
        vt = jnp.concatenate(
            [
                kv[1, s0, 0:HEAD, :], kv[1, s0, HEAD : 2 * HEAD, :],
                kv[1, s0 + 1, 0:HEAD, :], kv[1, s0 + 1, HEAD : 2 * HEAD, :],
            ],
            axis=1,
        )
        vt = jnp.concatenate([vt, ones], axis=0)
        scores = [dot(keys, qp[t], NT) for t in range(4)]
        for t in range(4):
            s = scores[t]
            if fresh:
                kpos = lax.broadcasted_iota(jnp.int32, s.shape, 0)
                qpos = lax.broadcasted_iota(jnp.int32, s.shape, 1) + c * tok
                s = jnp.where(kpos <= qpos, s, -1e30)
                new_max = jnp.max(s, axis=0, keepdims=True)
                w = jnp.where(kpos <= qpos, jnp.exp(s - new_max), 0.0).astype(bf16)
                acc[t] = dot(vt, w)
            else:
                old_max = mrow[t]
                new_max = jnp.maximum(old_max, jnp.max(s, axis=0, keepdims=True))
                w = jnp.exp(s - new_max).astype(bf16)
                acc[t] = acc[t] * jnp.exp(old_max - new_max) + dot(vt, w)
            mrow[t] = new_max

    def forward_w(d, u, v):
        i = w_item(d, u, v)

        @pl.when((i >= 1) & (i <= w_far[d]))
        def _():
            s = chip_from(d, i) * 2 + c
            piece = wbuf.at[0, s]
            got(piece, wz_sem.at[d, i])

            @pl.when((i < w_far[d]) & ((z > 0) | (u >= meet) | (d == 0)))
            def _():
                send_w(d, i)

            send(piece, wbuf.at[3, s], s_wx, wx_sem.at[1, d, i], xdev(1))
            send(piece, wbuf.at[1, s], s_wx, wx_sem.at[0, d, i], xdev(-1))
            send(piece, piece, s_wp, wp_sem.at[0], partner)

    def spread_w(d, u, v):
        j = w_item(d, u - 2, v)

        @pl.when((j >= d) & (j <= w_far[d]) & (u >= 2))
        def _():
            s = chip_from(d, j) * 2 + c
            for k in range(2):
                ref = wbuf.at[2 * k + 1, s]
                got(ref, wx_sem.at[k, d, j])
                send(ref, ref, s_wp, wp_sem.at[0], partner)
            send(wbuf.at[3 - 2 * c, s], wbuf.at[2, s], s_wr, wr_sem.at[d, j], xdev(1 - 2 * c))

        q = w_item(d, u - 4, v)

        @pl.when((q >= d) & (q <= w_far[d]) & (u >= 4))
        def _():
            ref = wbuf.at[2, chip_from(d, q) * 2 + c]
            got(ref, wr_sem.at[d, q])
            send(ref, ref, s_wp, wp_sem.at[0], partner)

    def forward_kv(d, u, kind):
        i = item(d, u)

        @pl.when(kv_in(d, i))
        def _():
            piece = kv.at[kind, chip_from(d, i) * 2 + c]
            got(piece, kvz_sem.at[d, i, kind])

            @pl.when(kv_out(d, i) & ((z > 0) | (u >= meet) | (d == 0)))
            def _():
                send_kv(d, i, kind)

            @pl.when(kv_used(d, i))
            def _():
                send(piece, piece, skp_sem.at[d, i, kind], kvp_sem.at[d, i, kind], partner)

    def take(d, u):
        i = item(d, u - 1)

        @pl.when(kv_used(d, i) & (u >= 1))
        def _():
            chip = chip_from(d, i)
            for kind in range(2):
                got(kv.at[kind, chip * 2 + 1 - c], kvp_sem.at[d, i, kind])
            pair_update(chip, False)

    def meet_top(u):
        @pl.when((z == 0) & (u == meet))
        def _():
            pl.semaphore_wait(wrap_ready, 1)

            def late(k, carry):
                send_w(1, k)
                for kind in range(2):

                    @pl.when(kv_out(1, k))
                    def _():
                        send_kv(1, k, kind)

                return carry

            lax.fori_loop(0, meet, late, 0)

    def hand_out(src, which):
        for r in range(1, 4):
            d = (x - r + ntp) % ntp
            rows = src.at[pl.ds(pl.multiple_of(d * rows_out, rows_out), rows_out)]
            send(rows, ract.at[which, r], s_act, act_sem.at[which, r], (g, sp, d))

    late_turn = half + jnp.maximum((z - half - HOPS) // HOPS, 0)
    turn = jnp.where(z < half, z + 1, late_turn)

    def state_steps(i):
        @pl.when((i >= 1) & (i <= HOPS) & (z >= i))
        def _():
            got(tm.at[i], st_sem.at[i])

            @pl.when((i < HOPS) & (z < top))
            def _():
                send(tm.at[i], tm.at[i + 1], send_sem.at[9 + i], st_sem.at[i + 1], above)

        @pl.when(i == turn)
        def _():
            @pl.when(z >= HOPS)
            def _():
                got(ch.at[0], st_sem.at[HOPS + 1])

            state = unpack_state(ch[0])
            for r in range(HOPS, 0, -1):
                state = state * unpack_decay(tm[r]) + unpack_state(tm[r])
            ch[1, 0:HEAD, :] = state.astype(bf16)
            send(ch.at[1], pe, s_pe, st_sem.at[HOPS + 2], partner)

            @pl.when(z + HOPS <= top)
            def _():
                pl.semaphore_wait(chain_ready, 1)
                send(
                    ch.at[1], ch.at[0], s_chain, st_sem.at[HOPS + 1],
                    zdev(jnp.minimum(z + HOPS, top)),
                )

        @pl.when(i == turn + 1)
        def _():
            got(pe, st_sem.at[HOPS + 2])
            ours, theirs = unpack_state(ch[1]), unpack_state(pe[...])
            for h in range(2):
                cols = slice(h * HEAD, (h + 1) * HEAD)
                before = jnp.where(c == h, ours, theirs)
                second = before * unpack_decay(spart[h]) + unpack_state(spart[h])
                before = jnp.where(up, before, second).astype(bf16)
                mix = loc[:, cols] + dot(qe[:, cols], before, NT)
                mean_square = jnp.mean(mix * mix, axis=-1, keepdims=True)
                arec[:, cols] = (mix * lax.rsqrt(mean_square + EPS) * rgain[...]).astype(bf16)
            hand_out(arec, 0)

    def step(u, carry):
        meet_top(u)
        for d, v in ((0, 0), (1, 0), (0, 1)):
            forward_w(d, u, v)
        for d in range(2):
            forward_kv(d, u, 0)
        state_steps(u)
        take(0, u)
        for d in range(2):
            forward_kv(d, u, 1)
        for d, v in ((0, 0), (1, 0), (0, 1)):
            spread_w(d, u, v)
        take(1, u)

        @pl.when(u == 0)
        def _():
            local_outputs()
            for kind in range(2):
                got(kv.at[kind, z * 2 + 1 - c], kvo_sem.at[kind])
            pair_update(z, True)

        return carry

    lax.fori_loop(0, half + 8, step, 0)

    for h in range(2):
        cols = slice(h * HEAD, (h + 1) * HEAD)
        first, second = acc[h], acc[2 + h]
        mix = first[0:HEAD] / first[HEAD : HEAD + 1]
        mix = mix - lam[h : h + 1, 0:1] * (second[0:HEAD] / second[HEAD : HEAD + 1])
        mean_square = jnp.mean(mix * mix, axis=0, keepdims=True)
        mix = jnp.transpose(mix * lax.rsqrt(mean_square + EPS))
        aatt[:, cols] = (mix * again[...]).astype(bf16)
    hand_out(aatt, 1)

    got(wbuf.at[0:4, 0:nz], wp_sem.at[0])
    chunk = 512
    pieces = chunk // 32

    def project(which, src):
        own_rows = src[pl.ds(pl.multiple_of(x * rows_out, rows_out), rows_out), :]
        acts = [own_rows if r == 0 else ract[which, r] for r in range(4)]

        def columns(n):
            total = None
            for r in range(4):
                w = [
                    wbuf[
                        r, pl.ds(n * pieces, pieces),
                        which * 64 + kb * 32 : which * 64 + kb * 32 + 32, :
                    ].reshape(chunk, HEAD)
                    for kb in range(2)
                ]
                term = dot(acts[r], jnp.concatenate(w, axis=1), NT)
                total = term if total is None else total + term
            return total

        return columns

    for r in range(1, 4):
        got(ract.at[0, r], act_sem.at[0, r])
    rec = project(0, arec)
    for n in range(2048 // chunk):
        part[:, n * chunk : (n + 1) * chunk] = rec(n)
    for r in range(1, 4):
        got(ract.at[1, r], act_sem.at[1, r])
    att = project(1, aatt)
    for n in range(2048 // chunk):
        cols = slice(n * chunk, (n + 1) * chunk)
        out[:, cols] = (part[:, cols] + att(n)).astype(bf16)

    def drain(i, carry):
        for d in range(2):
            for kind in range(2):

                @pl.when(kv_out(d, i))
                def _():
                    got(kv.at[kind, 0], skz_sem.at[d, i, kind])

                @pl.when(kv_used(d, i))
                def _():
                    got(kv.at[kind, 0], skp_sem.at[d, i, kind])

        return carry

    lax.fori_loop(0, kv_up + 1, drain, 0)
    for kind in range(2):
        got(kv.at[kind, 0], s_kvo[kind])
    got(wbuf.at[0, 0 : nz - 1], s_wz)
    got(wbuf.at[0:2, 0:nz], s_wx)
    got(wbuf.at[0, 0:nz], s_wr)
    got(wbuf.at[0:4, 0:nz], s_wp)
    got(sown, s_own)
    got(pe, s_pe)

    @pl.when(z + HOPS <= top)
    def _():
        got(pe, s_chain)

    for r in range(HOPS):

        @pl.when((z < top) & (z >= r))
        def _():
            got(pe, s_tm[r])

    got(ract.at[0:2, 1:4], s_act)


def shards(rq, fg, rv, lb, added, rgain, q1, k1, q2, k2, v, lam, again, w, *, nz):
    tok = rq.shape[0]
    half_tok = tok // 2
    keys = jnp.concatenate([k1, k2], axis=1)
    vt = v.reshape(2, half_tok, HEAD).transpose(0, 2, 1).reshape(tok, HEAD)
    kvl = jnp.stack([keys, vt])
    wl = w.reshape(2, 2, HEAD, 32).transpose(0, 1, 3, 2).reshape(HEAD, HEAD)
    scale = jnp.asarray(DA_HD**-0.5, bf16)
    zero = jnp.zeros((tok, DA_HD), bf16)
    qp = jnp.stack(
        [
            jnp.concatenate([q1[:, :DA_HD] * scale, zero], axis=1),
            jnp.concatenate([q1[:, DA_HD:] * scale, zero], axis=1),
            jnp.concatenate([zero, q2[:, :DA_HD] * scale], axis=1),
            jnp.concatenate([zero, q2[:, DA_HD:] * scale], axis=1),
        ]
    )
    vmem = pl.BlockSpec(memory_space=pltpu.VMEM)
    hbm = pl.BlockSpec(memory_space=pltpu.HBM)
    nsp = 2 * nz
    msg = (HEAD + 16, HEAD)
    dma = pltpu.SemaphoreType.DMA
    return pl.pallas_call(
        functools.partial(kernel, nz),
        out_shape=jax.ShapeDtypeStruct((tok // 4, w.shape[2] * nsp), bf16),
        in_specs=[hbm] * 6 + [vmem] * 5,
        out_specs=vmem,
        scratch_shapes=[
            pltpu.VMEM((4, tok, HEAD), bf16),
            pltpu.VMEM((tok, 2 * HEAD), bf16),
            pltpu.VMEM((tok, 2 * HEAD), bf16),
            pltpu.VMEM((tok, 2 * HEAD), bf16),
            pltpu.VMEM((2, nsp, tok, HEAD), bf16),
            pltpu.VMEM((4, nsp, HEAD, HEAD), bf16),
            pltpu.VMEM((4, HEAD + 16, tok), f32),
            pltpu.VMEM((4, 1, tok), f32),
            pltpu.VMEM((2,) + msg, bf16),
            pltpu.VMEM((2,) + msg, bf16),
            pltpu.VMEM((HOPS + 1,) + msg, bf16),
            pltpu.VMEM((2,) + msg, bf16),
            pltpu.VMEM(msg, bf16),
            pltpu.VMEM((tok, 2 * HEAD), f32),
            pltpu.VMEM((tok, 2 * HEAD), bf16),
            pltpu.VMEM((2, HEAD, HEAD), f32),
            pltpu.VMEM((2, 1, HEAD), f32),
            pltpu.VMEM((tok, 2 * HEAD), bf16),
            pltpu.VMEM((tok, 2 * HEAD), bf16),
            pltpu.VMEM((2, 4, tok // 4, 2 * HEAD), bf16),
            pltpu.VMEM((tok // 4, w.shape[2] * nsp), f32),
            dma((7,)),
            dma((11 + HOPS,)),
            dma((2, (21 * nz) // 32 + 2, 2)),
            dma((2, (21 * nz) // 32 + 2, 2)),
            dma((2, (21 * nz) // 32 + 2, 2)),
            dma((2, (21 * nz) // 32 + 2, 2)),
            dma((2,)),
            dma((2, nz // 2 + 2)),
            dma((2, 2, nz // 2 + 1)),
            dma((2, nz // 2 + 1)),
            dma((1,)),
            dma((HOPS + 3,)),
            dma((2, 4)),
            pltpu.SemaphoreType.REGULAR,
            pltpu.SemaphoreType.REGULAR,
        ],
        compiler_params=pltpu.CompilerParams(
            collective_id=0, has_side_effects=True, vmem_limit_bytes=60 * 1024 * 1024
        ),
    )(
        kvl, wl, qp, rq, fg, rv, lb.reshape(1, -1), added,
        jnp.broadcast_to(lam[:, None], (2, HEAD)), rgain.reshape(1, -1), again.reshape(1, -1),
    )


def solution(mesh):
    tokens = P(("grp", "sp"), "tp")
    return jax.shard_map(
        functools.partial(shards, nz=mesh.shape["sp"] // 2),
        mesh=mesh,
        in_specs=(
            tokens, tokens, tokens, P("tp"), tokens, P(),
            tokens, tokens, tokens, tokens, tokens, P("tp"), P(), P(None, "tp", "sp"),
        ),
        out_specs=P(("grp", "sp", "tp"), None),
        check_vma=False,
    )
```

```python
import functools

import jax
import jax.numpy as jnp
from jax import lax
from jax.experimental import pallas as pl
from jax.experimental.pallas import tpu as pltpu
from jax.sharding import PartitionSpec as P

HEAD = 128
DA_HD = 64
BLK = 64
HOPS = 4
EPS = 1e-06
f32, bf16 = jnp.float32, jnp.bfloat16
NT = (((1,), (1,)), ((), ()))
TN = (((0,), (0,)), ((), ()))


def dot(a, b, dims=(((1,), (0,)), ((), ())), precision=None):
    return lax.dot_general(a, b, dims, precision=precision, preferred_element_type=f32)


def kernel(
    nz, kvl, wl, qp_in, rq_in, fg_in, rv_in, lb, added, lam, rgain, again, out,
    qp, rq, fg, rv,
    kv, wbuf, acc, mrow, sown, spart, tm, ch, pe, loc, qe, dev_state, dev_decay,
    arec, aatt, ract, part,
    copy_sem, send_sem, skz_sem, skp_sem, kvz_sem, kvp_sem, kvo_sem, wz_sem, wx_sem, wr_sem,
    wp_sem, st_sem, act_sem, chain_ready, wrap_ready,
):
    g, sp, x = lax.axis_index("grp"), lax.axis_index("sp"), lax.axis_index("tp")
    ntp = lax.axis_size("tp")
    z, c = sp // 2, sp % 2
    up = c == 0
    top = nz - 1
    half = nz // 2
    kv_up = (21 * nz) // 32
    kv_wrap = nz - 1 - kv_up
    w_far = (half, half - 1)
    gap = jnp.maximum(1 - z, 0)
    meet = 1
    tok = rq.shape[0]
    rows_out = tok // ntp
    mesh_id = pl.DeviceIdType.MESH

    def zdev(chip):
        return (g, chip * 2 + c, x)

    def xdev(dx):
        return (g, sp, (x + dx + ntp) % ntp)

    partner = (g, z * 2 + 1 - c, x)
    ring = (zdev((z + 1) % nz), zdev((z - 1 + nz) % nz))

    def send(src, dst, s_sem, r_sem, to):
        pltpu.make_async_remote_copy(
            src_ref=src, dst_ref=dst, send_sem=s_sem, recv_sem=r_sem,
            device_id=to, device_id_type=mesh_id,
        ).start()

    def got(ref, sem):
        pltpu.make_async_copy(ref, ref, sem).wait()

    def tell(sem, dev):
        pl.semaphore_signal(sem, inc=1, device_id=dev, device_id_type=mesh_id)

    def chip_from(d, i):
        return (z - i + nz) % nz if d == 0 else (z + i) % nz

    def item(d, u):
        if d == 1:
            return u
        return jnp.where(u <= z, u, jnp.where(u > z + gap, u - gap, -1))

    def w_item(d, u, v):
        if d == 1:
            return u if v == 0 else jnp.int32(-1)
        low = item(0, u) if v == 0 else jnp.int32(-1)
        low = jnp.where(u > z + gap, z + 2 * (u - z - gap) - 1 + v, low)
        near = z - half
        steps = (near + 1) // 2
        fast = jnp.where((u >= 1) & (2 * u - 1 + v <= near), 2 * u - 1 + v, u if v == 0 else -1)
        fast = jnp.where((u >= 1) & (v == 1) & (2 * u > near), -1, fast)
        slow = near + u - steps if v == 0 else jnp.int32(-1)
        high = jnp.where(u <= steps, fast, slow)
        return jnp.where(z < half, low, high)

    def kv_used(d, i):
        if d == 0:
            return (i >= 1) & (i <= kv_up) & (z >= i)
        return (i >= 1) & (i <= kv_wrap) & (z + i >= nz)

    def kv_in(d, i):
        if d == 0:
            return kv_used(0, i)
        return kv_used(1, i) | (i >= 1) & (z + i < kv_wrap)

    def kv_out(d, i):
        own = z < (top if d == 0 else kv_wrap)
        on = (z < top) & (i < kv_up) if d == 0 else i < kv_wrap
        return (i == 0) & own | kv_in(d, i) & on

    def kv_pair(kind, chip):
        return kv.at[kind, pl.ds(2 * chip, 2)]

    loads = [pltpu.make_async_copy(kvl.at[k], kv.at[k, sp], copy_sem.at[k]) for k in range(2)]
    loads.append(pltpu.make_async_copy(wl, wbuf.at[0, sp], copy_sem.at[2]))
    for k, (src, dst) in enumerate(((fg_in, fg), (rv_in, rv), (rq_in, rq), (qp_in, qp))):
        loads.append(pltpu.make_async_copy(src, dst, copy_sem.at[3 + k]))
    for load in loads:
        load.start()
    tm[...] = jnp.zeros_like(tm)
    ch[...] = jnp.zeros_like(ch)

    barrier = pltpu.get_barrier_semaphore()

    def greet(cond, dev):
        @pl.when(cond)
        def _():
            tell(barrier, dev)

    for dx in range(1, 4):
        tell(barrier, xdev(dx))
    tell(barrier, partner)
    greet(z < top, zdev(jnp.minimum(z + 1, top)))
    greet(z > 0, zdev(jnp.maximum(z - 1, 0)))
    greet(z + HOPS <= top, zdev(jnp.minimum(z + HOPS, top)))
    greet(z == 0, zdev(top))
    one = jnp.int32(1)
    none = jnp.int32(0)
    callers = 4 + jnp.where(z < top, one, none) + jnp.where(z > 0, one, none)
    callers = callers + jnp.where(z >= HOPS, one, none)
    callers = callers + jnp.where(z == top, one, none)
    pl.semaphore_wait(barrier, callers)

    @pl.when(z >= HOPS)
    def _():
        tell(chain_ready, zdev(jnp.maximum(z - HOPS, 0)))

    @pl.when(z == top)
    def _():
        tell(wrap_ready, zdev(0))

    s_wz, s_wx, s_wr, s_wp, s_act, s_own, s_chain, s_pe = (send_sem.at[k] for k in range(8))
    s_tm = [send_sem.at[9 + r] for r in range(HOPS)]
    s_kvo = [send_sem.at[9 + HOPS + k] for k in range(2)]

    def send_kv(d, i, kind):
        piece = kv.at[kind, chip_from(d, i) * 2 + c]
        send(piece, piece, skz_sem.at[d, i, kind], kvz_sem.at[d, i + 1, kind], ring[d])

    def send_w(d, i):
        piece = wbuf.at[0, chip_from(d, i) * 2 + c]
        send(piece, piece, s_wz, wz_sem.at[d, i + 1], ring[d])

    loads[0].wait()
    loads[1].wait()
    for kind in range(2):
        for d in range(2):

            @pl.when(kv_out(d, 0) & ((z > 0) | (d == 0)))
            def _():
                send_kv(d, jnp.int32(0), kind)

        mine = kv.at[kind, sp]
        send(mine, mine, s_kvo[kind], kvo_sem.at[kind], partner)
    loads[2].wait()
    mine = wbuf.at[0, sp]
    send_w(0, jnp.int32(0))

    @pl.when(z > 0)
    def _():
        send_w(1, jnp.int32(0))

    send(mine, mine, s_wp, wp_sem.at[0], partner)
    send(mine, wbuf.at[3, sp], s_wx, wx_sem.at[1, 0, 0], xdev(1))
    send(mine, wbuf.at[1, sp], s_wx, wx_sem.at[0, 0, 0], xdev(-1))

    for load in loads[3:]:
        load.wait()
    floor_rate = jax.nn.sigmoid(-lb[...])
    inflow = floor_rate * jax.nn.sigmoid(-fg[...].astype(f32))
    one_less = 1.0 - inflow
    add2 = added[...]
    add_wide = jnp.concatenate(
        [jnp.broadcast_to(add2[:, h : h + 1], (tok, HEAD)) for h in range(2)], axis=1
    )
    log_decay = jnp.log(one_less) - ((one_less - 1.0) + inflow) / one_less + add_wide
    row = lax.broadcasted_iota(jnp.int32, (tok, tok), 0)
    col = lax.broadcasted_iota(jnp.int32, (tok, tok), 1)
    tri = jnp.where(col <= row, 1.0, 0.0).astype(f32)
    cum = dot(tri, log_decay, precision=lax.Precision.HIGHEST)
    last = cum[tok - 1 : tok, :]
    kin = (inflow * jnp.exp(last - cum)).astype(bf16)
    through = jnp.exp(last)
    r16 = lax.broadcasted_iota(jnp.int32, (16, HEAD), 0)

    def pack_decay(dec):
        hi = dec.astype(bf16)
        lo = (dec - hi.astype(f32)).astype(bf16)
        zero = jnp.zeros((16, HEAD), f32)
        return jnp.where(
            r16 == 0, hi.astype(f32), jnp.where(r16 == 1, lo.astype(f32), zero)
        ).astype(bf16)

    def unpack_decay(msg):
        rows = msg[HEAD : HEAD + 16, :].astype(f32)
        return rows[0:1] + rows[1:2]

    def unpack_state(msg):
        return msg[0:HEAD, :].astype(f32)

    for h in range(2):
        cols = slice(h * HEAD, (h + 1) * HEAD)
        st = dot(rv[:, cols], kin[:, cols], TN)
        dev_state[h] = st
        dev_decay[h] = through[:, cols]
        sown[h, 0:HEAD, :] = st.astype(bf16)
        sown[h, HEAD : HEAD + 16, :] = pack_decay(through[:, cols])
    send(sown, spart, s_own, st_sem.at[0], partner)

    got(spart, st_sem.at[0])
    own_s, own_d = dev_state[c], dev_decay[c]
    oth_s, oth_d = unpack_state(spart[c]), unpack_decay(spart[c])
    late_d = jnp.where(up, oth_d, own_d)
    chip_state = late_d * jnp.where(up, own_s, oth_s) + jnp.where(up, oth_s, own_s)
    tm[0, 0:HEAD, :] = chip_state.astype(bf16)
    tm[0, HEAD : HEAD + 16, :] = pack_decay(own_d * oth_d)
    above = zdev(jnp.minimum(z + 1, top))

    @pl.when(z < top)
    def _():
        send(tm.at[0], tm.at[1], s_tm[0], st_sem.at[1], above)

    qe[...] = (rq[...].astype(f32) * jnp.exp(cum)).astype(bf16)

    def local_outputs():
        r64 = lax.broadcasted_iota(jnp.int32, (BLK, BLK), 0)
        c64 = lax.broadcasted_iota(jnp.int32, (BLK, BLK), 1)
        for h in range(2):
            cols = slice(h * HEAD, (h + 1) * HEAD)
            state = None
            for b in range(tok // BLK):
                rows = slice(b * BLK, (b + 1) * BLK)
                blk_cum = cum[rows, cols]
                if b:
                    blk_cum = blk_cum - cum[b * BLK - 1 : b * BLK, cols]
                qd = (rq[rows, cols].astype(f32) * jnp.exp(blk_cum)).astype(bf16)
                kd = (inflow[rows, cols] * jnp.exp(-blk_cum)).astype(bf16)
                scores = dot(qd, kd, NT)
                scores = jnp.where(c64 <= r64, scores, 0.0).astype(bf16)
                res = dot(scores, rv[rows, cols])
                if b:
                    res = res + dot(qd, state.astype(bf16), NT)
                loc[rows, cols] = res
                if b + 1 < tok // BLK:
                    end = blk_cum[BLK - 1 : BLK, :]
                    ke = (inflow[rows, cols] * jnp.exp(end - blk_cum)).astype(bf16)
                    new = dot(rv[rows, cols], ke, TN)
                    state = new if b == 0 else state * jnp.exp(end) + new

    ones = jnp.ones((16, 2 * tok), bf16)

    def pair_update(chip, fresh):
        s0 = chip * 2
        keys = kv[0, pl.ds(s0, 2)].reshape(2 * tok, HEAD)
        vt = jnp.concatenate(
            [
                kv[1, s0, 0:HEAD, :], kv[1, s0, HEAD : 2 * HEAD, :],
                kv[1, s0 + 1, 0:HEAD, :], kv[1, s0 + 1, HEAD : 2 * HEAD, :],
            ],
            axis=1,
        )
        vt = jnp.concatenate([vt, ones], axis=0)
        scores = [dot(keys, qp[t], NT) for t in range(4)]
        for t in range(4):
            s = scores[t]
            if fresh:
                kpos = lax.broadcasted_iota(jnp.int32, s.shape, 0)
                qpos = lax.broadcasted_iota(jnp.int32, s.shape, 1) + c * tok
                s = jnp.where(kpos <= qpos, s, -1e30)
                new_max = jnp.max(s, axis=0, keepdims=True)
                w = jnp.where(kpos <= qpos, jnp.exp(s - new_max), 0.0).astype(bf16)
                acc[t] = dot(vt, w)
            else:
                old_max = mrow[t]
                new_max = jnp.maximum(old_max, jnp.max(s, axis=0, keepdims=True))
                w = jnp.exp(s - new_max).astype(bf16)
                acc[t] = acc[t] * jnp.exp(old_max - new_max) + dot(vt, w)
            mrow[t] = new_max

    def forward_w(d, u, v):
        i = w_item(d, u, v)

        @pl.when((i >= 1) & (i <= w_far[d]))
        def _():
            s = chip_from(d, i) * 2 + c
            piece = wbuf.at[0, s]
            got(piece, wz_sem.at[d, i])

            @pl.when((i < w_far[d]) & ((z > 0) | (u >= meet) | (d == 0)))
            def _():
                send_w(d, i)

            send(piece, wbuf.at[3, s], s_wx, wx_sem.at[1, d, i], xdev(1))
            send(piece, wbuf.at[1, s], s_wx, wx_sem.at[0, d, i], xdev(-1))
            send(piece, piece, s_wp, wp_sem.at[0], partner)

    def spread_w(d, u, v):
        j = w_item(d, u - 2, v)

        @pl.when((j >= d) & (j <= w_far[d]) & (u >= 2))
        def _():
            s = chip_from(d, j) * 2 + c
            for k in range(2):
                ref = wbuf.at[2 * k + 1, s]
                got(ref, wx_sem.at[k, d, j])
                send(ref, ref, s_wp, wp_sem.at[0], partner)
            send(wbuf.at[3 - 2 * c, s], wbuf.at[2, s], s_wr, wr_sem.at[d, j], xdev(1 - 2 * c))

        q = w_item(d, u - 4, v)

        @pl.when((q >= d) & (q <= w_far[d]) & (u >= 4))
        def _():
            ref = wbuf.at[2, chip_from(d, q) * 2 + c]
            got(ref, wr_sem.at[d, q])
            send(ref, ref, s_wp, wp_sem.at[0], partner)

    def forward_kv(d, u, kind):
        i = item(d, u)

        @pl.when(kv_in(d, i))
        def _():
            piece = kv.at[kind, chip_from(d, i) * 2 + c]
            got(piece, kvz_sem.at[d, i, kind])

            @pl.when(kv_out(d, i) & ((z > 0) | (u >= meet) | (d == 0)))
            def _():
                send_kv(d, i, kind)

            @pl.when(kv_used(d, i))
            def _():
                send(piece, piece, skp_sem.at[d, i, kind], kvp_sem.at[d, i, kind], partner)

    def take(d, u):
        i = item(d, u - 1)

        @pl.when(kv_used(d, i) & (u >= 1))
        def _():
            chip = chip_from(d, i)
            for kind in range(2):
                got(kv.at[kind, chip * 2 + 1 - c], kvp_sem.at[d, i, kind])
            pair_update(chip, False)

    def meet_top(u):
        @pl.when((z == 0) & (u == meet))
        def _():
            pl.semaphore_wait(wrap_ready, 1)

            def late(k, carry):
                send_w(1, k)
                for kind in range(2):

                    @pl.when(kv_out(1, k))
                    def _():
                        send_kv(1, k, kind)

                return carry

            lax.fori_loop(0, meet, late, 0)

    def hand_out(src, which):
        for r in range(1, 4):
            d = (x - r + ntp) % ntp
            rows = src.at[pl.ds(pl.multiple_of(d * rows_out, rows_out), rows_out)]
            send(rows, ract.at[which, r], s_act, act_sem.at[which, r], (g, sp, d))

    late_turn = half + jnp.maximum((z - half - HOPS) // HOPS, 0)
    turn = jnp.where(z < half, z + 1, late_turn)

    def state_steps(i):
        @pl.when((i >= 1) & (i <= HOPS) & (z >= i))
        def _():
            got(tm.at[i], st_sem.at[i])

            @pl.when((i < HOPS) & (z < top))
            def _():
                send(tm.at[i], tm.at[i + 1], send_sem.at[9 + i], st_sem.at[i + 1], above)

        @pl.when(i == turn)
        def _():
            @pl.when(z >= HOPS)
            def _():
                got(ch.at[0], st_sem.at[HOPS + 1])

            state = unpack_state(ch[0])
            for r in range(HOPS, 0, -1):
                state = state * unpack_decay(tm[r]) + unpack_state(tm[r])
            ch[1, 0:HEAD, :] = state.astype(bf16)
            send(ch.at[1], pe, s_pe, st_sem.at[HOPS + 2], partner)

            @pl.when(z + HOPS <= top)
            def _():
                pl.semaphore_wait(chain_ready, 1)
                send(
                    ch.at[1], ch.at[0], s_chain, st_sem.at[HOPS + 1],
                    zdev(jnp.minimum(z + HOPS, top)),
                )

        @pl.when(i == turn + 1)
        def _():
            got(pe, st_sem.at[HOPS + 2])
            ours, theirs = unpack_state(ch[1]), unpack_state(pe[...])
            for h in range(2):
                cols = slice(h * HEAD, (h + 1) * HEAD)
                before = jnp.where(c == h, ours, theirs)
                second = before * unpack_decay(spart[h]) + unpack_state(spart[h])
                before = jnp.where(up, before, second).astype(bf16)
                mix = loc[:, cols] + dot(qe[:, cols], before, NT)
                mean_square = jnp.mean(mix * mix, axis=-1, keepdims=True)
                arec[:, cols] = (mix * lax.rsqrt(mean_square + EPS) * rgain[...]).astype(bf16)
            hand_out(arec, 0)

    def finish_attention():
        for h in range(2):
            cols = slice(h * HEAD, (h + 1) * HEAD)
            first, second = acc[h], acc[2 + h]
            mix = first[0:HEAD] / first[HEAD : HEAD + 1]
            mix = mix - lam[0:1, h : h + 1] * (second[0:HEAD] / second[HEAD : HEAD + 1])
            mean_square = jnp.mean(mix * mix, axis=0, keepdims=True)
            mix = jnp.transpose(mix * lax.rsqrt(mean_square + EPS))
            aatt[:, cols] = (mix * again[...]).astype(bf16)
        hand_out(aatt, 1)

    final = jnp.minimum(z, kv_up) + 2

    def step(u, carry):
        meet_top(u)
        for d, v in ((0, 0), (1, 0), (0, 1)):
            forward_w(d, u, v)
        for d in range(2):
            forward_kv(d, u, 0)
        state_steps(u)
        take(0, u)
        for d in range(2):
            forward_kv(d, u, 1)
        for d, v in ((0, 0), (1, 0), (0, 1)):
            spread_w(d, u, v)
        take(1, u)

        @pl.when(u == 0)
        def _():
            local_outputs()
            for kind in range(2):
                got(kv.at[kind, z * 2 + 1 - c], kvo_sem.at[kind])
            pair_update(z, True)

        @pl.when(u == final)
        def _():
            finish_attention()

        return carry

    lax.fori_loop(0, half + 8, step, 0)

    got(wbuf.at[0:4, 0:nz], wp_sem.at[0])
    chunk = 512
    pieces = chunk // 32

    def project(which, src):
        own_rows = src[pl.ds(pl.multiple_of(x * rows_out, rows_out), rows_out), :]
        acts = [own_rows if r == 0 else ract[which, r] for r in range(4)]

        def columns(n):
            total = None
            for r in range(4):
                w = [
                    wbuf[
                        r, pl.ds(n * pieces, pieces),
                        which * 64 + kb * 32 : which * 64 + kb * 32 + 32, :
                    ].reshape(chunk, HEAD)
                    for kb in range(2)
                ]
                term = dot(acts[r], jnp.concatenate(w, axis=1), NT)
                total = term if total is None else total + term
            return total

        return columns

    for r in range(1, 4):
        got(ract.at[0, r], act_sem.at[0, r])
    rec = project(0, arec)
    for n in range(2048 // chunk):
        part[:, n * chunk : (n + 1) * chunk] = rec(n)
    for r in range(1, 4):
        got(ract.at[1, r], act_sem.at[1, r])
    att = project(1, aatt)
    for n in range(2048 // chunk):
        cols = slice(n * chunk, (n + 1) * chunk)
        out[:, cols] = (part[:, cols] + att(n)).astype(bf16)

    def drain(i, carry):
        for d in range(2):
            for kind in range(2):

                @pl.when(kv_out(d, i))
                def _():
                    got(kv.at[kind, 0], skz_sem.at[d, i, kind])

                @pl.when(kv_used(d, i))
                def _():
                    got(kv.at[kind, 0], skp_sem.at[d, i, kind])

        return carry

    lax.fori_loop(0, kv_up + 1, drain, 0)
    for kind in range(2):
        got(kv.at[kind, 0], s_kvo[kind])
    got(wbuf.at[0, 0 : nz - 1], s_wz)
    got(wbuf.at[0:2, 0:nz], s_wx)
    got(wbuf.at[0, 0:nz], s_wr)
    got(wbuf.at[0:4, 0:nz], s_wp)
    got(sown, s_own)
    got(pe, s_pe)

    @pl.when(z + HOPS <= top)
    def _():
        got(pe, s_chain)

    for r in range(HOPS):

        @pl.when((z < top) & (z >= r))
        def _():
            got(pe, s_tm[r])

    got(ract.at[0:2, 1:4], s_act)


def shards(rq, fg, rv, lb, added, rgain, q1, k1, q2, k2, v, lam, again, w, *, nz):
    tok = rq.shape[0]
    half_tok = tok // 2
    keys = jnp.concatenate([k1, k2], axis=1)
    vt = v.reshape(2, half_tok, HEAD).transpose(0, 2, 1).reshape(tok, HEAD)
    kvl = jnp.stack([keys, vt])
    wl = w.reshape(2, 2, HEAD, 32).transpose(0, 1, 3, 2).reshape(HEAD, HEAD)
    scale = jnp.asarray(DA_HD**-0.5, bf16)
    zero = jnp.zeros((tok, DA_HD), bf16)
    qp = jnp.stack(
        [
            jnp.concatenate([q1[:, :DA_HD] * scale, zero], axis=1),
            jnp.concatenate([q1[:, DA_HD:] * scale, zero], axis=1),
            jnp.concatenate([zero, q2[:, :DA_HD] * scale], axis=1),
            jnp.concatenate([zero, q2[:, DA_HD:] * scale], axis=1),
        ]
    )
    vmem = pl.BlockSpec(memory_space=pltpu.VMEM)
    hbm = pl.BlockSpec(memory_space=pltpu.HBM)
    nsp = 2 * nz
    msg = (HEAD + 16, HEAD)
    dma = pltpu.SemaphoreType.DMA
    return pl.pallas_call(
        functools.partial(kernel, nz),
        out_shape=jax.ShapeDtypeStruct((tok // 4, w.shape[2] * nsp), bf16),
        in_specs=[hbm] * 6 + [vmem] * 5,
        out_specs=vmem,
        scratch_shapes=[
            pltpu.VMEM((4, tok, HEAD), bf16),
            pltpu.VMEM((tok, 2 * HEAD), bf16),
            pltpu.VMEM((tok, 2 * HEAD), bf16),
            pltpu.VMEM((tok, 2 * HEAD), bf16),
            pltpu.VMEM((2, nsp, tok, HEAD), bf16),
            pltpu.VMEM((4, nsp, HEAD, HEAD), bf16),
            pltpu.VMEM((4, HEAD + 16, tok), f32),
            pltpu.VMEM((4, 1, tok), f32),
            pltpu.VMEM((2,) + msg, bf16),
            pltpu.VMEM((2,) + msg, bf16),
            pltpu.VMEM((HOPS + 1,) + msg, bf16),
            pltpu.VMEM((2,) + msg, bf16),
            pltpu.VMEM(msg, bf16),
            pltpu.VMEM((tok, 2 * HEAD), f32),
            pltpu.VMEM((tok, 2 * HEAD), bf16),
            pltpu.VMEM((2, HEAD, HEAD), f32),
            pltpu.VMEM((2, 1, HEAD), f32),
            pltpu.VMEM((tok, 2 * HEAD), bf16),
            pltpu.VMEM((tok, 2 * HEAD), bf16),
            pltpu.VMEM((2, 4, tok // 4, 2 * HEAD), bf16),
            pltpu.VMEM((tok // 4, w.shape[2] * nsp), f32),
            dma((7,)),
            dma((11 + HOPS,)),
            dma((2, (21 * nz) // 32 + 2, 2)),
            dma((2, (21 * nz) // 32 + 2, 2)),
            dma((2, (21 * nz) // 32 + 2, 2)),
            dma((2, (21 * nz) // 32 + 2, 2)),
            dma((2,)),
            dma((2, nz // 2 + 2)),
            dma((2, 2, nz // 2 + 1)),
            dma((2, nz // 2 + 1)),
            dma((1,)),
            dma((HOPS + 3,)),
            dma((2, 4)),
            pltpu.SemaphoreType.REGULAR,
            pltpu.SemaphoreType.REGULAR,
        ],
        compiler_params=pltpu.CompilerParams(
            collective_id=0, has_side_effects=True, vmem_limit_bytes=60 * 1024 * 1024
        ),
    )(
        kvl, wl, qp, rq, fg, rv, lb.reshape(1, -1), added,
        lam.reshape(1, -1), rgain.reshape(1, -1), again.reshape(1, -1),
    )


def solution(mesh):
    tokens = P(("grp", "sp"), "tp")
    return jax.shard_map(
        functools.partial(shards, nz=mesh.shape["sp"] // 2),
        mesh=mesh,
        in_specs=(
            tokens, tokens, tokens, P("tp"), tokens, P(),
            tokens, tokens, tokens, tokens, tokens, P("tp"), P(), P(None, "tp", "sp"),
        ),
        out_specs=P(("grp", "sp", "tp"), None),
        check_vma=False,
    )
```
